32 devices in a mesh: sp: 8 (over z, y), dp: 4 (over x, core).
Axes of the slice: x: 2, y: 2, z: 4, core: 2. Of those that a mesh axis runs over, the one named last changes fastest.
Arguments:
- residual: bfloat16 [4, 1024, 2048], P('dp', 'sp'), may hold values from -6 to 6
- head_input: bfloat16 [4, 1024, 2048], P('dp', 'sp'), may hold values from -6 to 6
- gate_input: bfloat16 [4, 1024, 2048], P('dp', 'sp'), may hold values from -6 to 6
- b_input: bfloat16 [4, 1024, 1024], P('dp', 'sp'), may hold values from -6 to 6
- c_input: bfloat16 [4, 1024, 1024], P('dp', 'sp'), may hold values from -6 to 6
- step_input: bfloat16 [4, 1024, 32], P('dp', 'sp'), may hold values from -4.8 to 4.8
- conv_weight: bfloat16 [4, 2048], replicated, may hold values from -3 to 3
- conv_b_weight: bfloat16 [4, 1024], replicated, may hold values from -3 to 3
- conv_c_weight: bfloat16 [4, 1024], replicated, may hold values from -3 to 3
- step_bias: float32 [32], replicated, may hold values from -1 to 1
- decay_log: float32 [32], replicated, may hold values from -9.92 to -2.99
- skip: float32 [32], replicated, may hold values from 0.5 to 1.5
- norm_gain: float32 [2048], replicated, may hold values from 0.1 to 1.9
- out_weight: bfloat16 [2048, 2048], P('dp'), may hold values from -0.125 to 0.125
- ffn_gain: float32 [2048], replicated, may hold values from 0.1 to 1.9
- shared_gate: bfloat16 [2048, 512], replicated, may hold values from -0.125 to 0.125
- shared_up: bfloat16 [2048, 512], replicated, may hold values from -0.125 to 0.125
- shared_down: bfloat16 [512, 2048], replicated, may hold values from -0.25 to 0.25
- expert_gate: bfloat16 [32, 2048, 512], P(('sp', 'dp')), may hold values from -0.125 to 0.125
- expert_up: bfloat16 [32, 2048, 512], P(('sp', 'dp')), may hold values from -0.125 to 0.125
- expert_down: bfloat16 [32, 512, 2048], P(('sp', 'dp')), may hold values from -0.25 to 0.25
- routes: int32 [4, 1024, 2], P('dp', 'sp'), may hold values from 0 to 31, all different within a row; in each aligned block of 128 rows (0 to 127, 128 to 255, ..., all dimensions but the last counted through in order) at most 16 rows name the same one
- route_weights: float32 [4, 1024, 2], P('dp', 'sp'), may hold values from 0.25 to 1.25
Outputs:
- layer_out: bfloat16 [4, 1024, 2048], P('dp', 'sp')
The draws below stay inside these ranges and needn't reach their ends.
Inputs may be any that keep to these rules, and one draw needn't show every extreme that they name: `routes`: each token names 2 different experts; among the rows of one device no expert is named more than 16 times, a bound that some block reaches.
All inputs are finite; a program needn't handle non-finite values.
Results may differ from the reference program's by a relative error of at most 0.015.
Values may be sent and summed in bfloat16 or wider, within the bound.
A program may use at most 128 MiB of HBM per device.

```python
import math
import jax
import jax.numpy as jnp
import numpy as np
from jax import lax

D = 2048
HEADS = 32
HEAD_DIM = 64
GROUPS = 8
STATE = 128
CONV_K = 4
BLOCK = 128
EXPERT_FF = 512
SHARED_FF = 512
TOP_K = 2
TOK_DEV = 128
INNER = 2048
SEQS = 4
LENGTH = 1024
EXPERTS = 32
CAP = 16
N_SP = 8
N_DP = 4


def draw_decay_log(key, part):
    first, second, third = jax.random.split(key, 3)
    share = 0.5
    quick = jax.random.uniform(first, (HEADS,), jnp.float32) < share
    slow = jax.random.uniform(second, (HEADS,), jnp.float32, math.log(5e-05), math.log(0.0002))
    fast = jax.random.uniform(third, (HEADS,), jnp.float32, math.log(0.015), math.log(0.05))
    return jnp.where(quick, fast, slow).astype(jnp.float32)


def draw_step_input(key, part):
    first, second = jax.random.split(key)
    count = LENGTH // TOK_DEV
    offset = jax.random.uniform(second, (SEQS, count, 1, HEADS), jnp.float32, -1.2, 1.2)
    noise = jnp.clip(jax.random.normal(first, (SEQS, count, TOK_DEV, HEADS), jnp.float32) * 0.6, -3.5, 3.5)
    return (offset + noise).reshape(SEQS, LENGTH, HEADS).astype(jnp.bfloat16)


def shard_levels(own_key, shape, pieces, least, largest):
    factor_of = 1.0
    for dim, blocks in pieces:
        steps = jax.random.uniform(jax.random.fold_in(jax.random.fold_in(own_key, 6), dim), (blocks,), jnp.float32, least / len(pieces), largest / len(pieces))
        factor_of = factor_of * jnp.repeat(jnp.exp(steps), shape[dim] // blocks).reshape((-1,) + (1,) * (len(shape) - 1 - dim))
    return factor_of


def routed_block(stream_key, own, number, rows, count, top, limit, slope):
    sequence = jax.random.permutation(stream_key, count)
    crowded, ordinary = load_shares(count, rows * top, limit, slope, True), load_shares(count, rows * top, limit, slope, False)
    places = jnp.arange(count)

    def named(lengths, rotation):
        used = int((lengths > 0).sum())
        fixed = max(1, used // 4)
        shifted = fixed + (places - fixed + rotation * (used - fixed)) % max(1, count - fixed)
        return jnp.zeros((count,), jnp.int32).at[sequence[jnp.where(places < fixed, places, shifted)]].set(jnp.asarray(lengths, jnp.int32))

    lengths = jnp.where(number % 4 == 0, named(crowded, number // 4), named(ordinary, number - number // 4 - 1))
    mixed = jax.random.permutation(jax.random.fold_in(own, 3), count)
    donor, receiver = mixed[0:count // 2 * 2:2], mixed[1:count // 2 * 2:2]
    room = jnp.minimum(lengths[donor] - 1, limit - lengths[receiver]) // 2
    room = jnp.where((donor == sequence[0]) | (receiver == sequence[0]) | (lengths[receiver] == 0), 0, jnp.maximum(room, 0))
    shifted = jax.random.randint(jax.random.fold_in(own, 4), (count // 2,), 0, 1 << 20) % (room + 1)
    lengths = lengths.at[donor].add(-shifted).at[receiver].add(shifted)
    labels = jnp.searchsorted(jnp.cumsum(lengths), jnp.arange(rows * top), side="right").astype(jnp.int32)
    listing = labels.reshape(top, rows).T
    listing = listing[jax.random.permutation(jax.random.fold_in(own, 1), rows)]
    rotation = jax.random.randint(jax.random.fold_in(own, 2), (rows, 1), 0, top)
    return jnp.take_along_axis(listing, (jnp.arange(top)[None, :] + rotation) % top, axis=1)


def load_shares(count, total, reach, slope, full):
    loads = [(1 << 20) // math.isqrt(rank ** slope) + 1 for rank in range(1, count + 1)]
    largest = reach if full else min(reach, max(-(-total // count), total * loads[0] // sum(loads)))
    least = 1 if total - largest >= count - 1 else 0
    given, rest = [largest] + [least] * (count - 1), total - largest - least * (count - 1)
    while rest > 0:
        movable = [i for i in range(1, count) if given[i] < largest] or [i for i in range(1, count) if given[i] < reach]
        pool, budget = sum([loads[i] for i in movable]), rest
        for i in movable:
            extra = min(reach - given[i], max(1, budget * loads[i] // pool), rest)
            given[i] = given[i] + extra
            rest = rest - extra
    return np.array(given)


def scatter_about(own_key, extent, scale, bound, pieces=(), kind=jnp.bfloat16):
    values = scale * jax.random.normal(own_key, extent, jnp.float32)
    if pieces:
        values = values * shard_levels(own_key, extent, pieces, -0.22, 0.18)
    return jnp.clip(values, -bound, bound).astype(kind)


def setup_inputs(seed: int = 0) -> dict:
    keys = jax.random.split(jax.random.key(seed), 24)
    residual = scatter_about(keys[0], (SEQS, LENGTH, D), 1.0, 6.0, ((0, 4), (1, 8)))
    head_input = scatter_about(keys[1], (SEQS, LENGTH, INNER), 1.0, 6.0, ((0, 4), (1, 8)))
    gate_input = scatter_about(keys[2], (SEQS, LENGTH, INNER), 1.0, 6.0, ((0, 4), (1, 8)))
    b_input = scatter_about(keys[3], (SEQS, LENGTH, GROUPS * STATE), 1.0, 6.0, ((0, 4), (1, 8)))
    c_input = scatter_about(keys[4], (SEQS, LENGTH, GROUPS * STATE), 1.0, 6.0, ((0, 4), (1, 8)))
    step_input = draw_step_input(jax.random.fold_in(keys[23], 71), 0)
    conv_weight = scatter_about(keys[6], (CONV_K, INNER), 0.5, 3.0)
    conv_b_weight = scatter_about(keys[7], (CONV_K, GROUPS * STATE), 0.5, 3.0)
    conv_c_weight = scatter_about(keys[8], (CONV_K, GROUPS * STATE), 0.5, 3.0)
    step_bias = jnp.clip(jax.random.uniform(keys[9], (HEADS,), jnp.float32, -1.0, 1.0), -1.0, 1.0)
    decay_log = draw_decay_log(jax.random.fold_in(keys[23], 71), 0)
    skip = jnp.clip(jax.random.uniform(keys[11], (HEADS,), jnp.float32, 0.5, 1.5), 0.5, 1.5)
    norm_gain = jnp.clip(1.0 + 0.18 * jax.random.normal(keys[12], (INNER,), jnp.float32), 0.1, 1.9)
    out_weight = scatter_about(keys[13], (INNER, D), INNER ** -0.5, 0.125, ((0, 4),))
    ffn_gain = jnp.clip(1.0 + 0.18 * jax.random.normal(keys[14], (D,), jnp.float32), 0.1, 1.9)
    shared_gate = scatter_about(keys[15], (D, SHARED_FF), D ** -0.5, 0.125)
    shared_up = scatter_about(keys[16], (D, SHARED_FF), D ** -0.5, 0.125)
    shared_down = scatter_about(keys[17], (SHARED_FF, D), SHARED_FF ** -0.5, 0.25)
    expert_gate = scatter_about(keys[18], (EXPERTS, D, EXPERT_FF), D ** -0.5, 0.125, ((0, 32),))
    expert_up = scatter_about(keys[19], (EXPERTS, D, EXPERT_FF), D ** -0.5, 0.125, ((0, 32),))
    expert_down = scatter_about(keys[20], (EXPERTS, EXPERT_FF, D), EXPERT_FF ** -0.5, 0.25, ((0, 32),))
    routes_keys = jax.random.split(jax.random.fold_in(keys[21], 1), SEQS * LENGTH // TOK_DEV)
    routes_turns = jax.random.permutation(jax.random.fold_in(keys[21], 3), SEQS * LENGTH // TOK_DEV)
    routes = jax.vmap(lambda own, number: routed_block(jax.random.fold_in(keys[21], 2), own, number, TOK_DEV, EXPERTS, TOP_K, CAP, 2))(routes_keys, routes_turns).reshape((SEQS, LENGTH, TOP_K))
    route_weights = jnp.clip(0.25 + 1.0 * jax.random.uniform(keys[22], (SEQS, LENGTH, TOP_K), jnp.float32) ** shard_levels(keys[22], (SEQS, LENGTH, TOP_K), ((0, 4), (1, 8)), -0.2, 0.2), 0.25, 1.25)
    return {"residual": residual, "head_input": head_input, "gate_input": gate_input, "b_input": b_input, "c_input": c_input, "step_input": step_input, "conv_weight": conv_weight, "conv_b_weight": conv_b_weight, "conv_c_weight": conv_c_weight, "step_bias": step_bias, "decay_log": decay_log, "skip": skip, "norm_gain": norm_gain, "out_weight": out_weight, "ffn_gain": ffn_gain, "shared_gate": shared_gate, "shared_up": shared_up, "shared_down": shared_down, "expert_gate": expert_gate, "expert_up": expert_up, "expert_down": expert_down, "routes": routes, "route_weights": route_weights}


EPS = 1e-06
HIGH = lax.Precision.HIGHEST

def conv_silu(padded, weight, length):
    total = jnp.zeros((length, padded.shape[1]), jnp.float32)
    for tap in range(weight.shape[0]):
        total = total + padded[tap:tap + length].astype(jnp.float32) * weight[tap].astype(jnp.float32)
    return jax.nn.silu(total)

def block_scan(xs, step, rate, bmat, cmat, block, init):
    length, heads, width = xs.shape
    count = length // block
    logs = (step * rate[None, :]).reshape(count, block, heads)
    weighted = (xs * step[:, :, None]).reshape(count, block, heads, width)
    bb = bmat.reshape(count, block, heads, -1)
    cc = cmat.reshape(count, block, heads, -1)
    cum = jnp.cumsum(logs, axis=1)
    lower = jnp.tril(jnp.ones((block, block), dtype=bool))[None, :, :, None]
    diff = cum[:, :, None, :] - cum[:, None, :, :]
    decay = jnp.where(lower, jnp.exp(jnp.where(lower, diff, 0.0)), 0.0)
    scores = jnp.einsum('clhn,cshn->clsh', cc, bb, precision=HIGH) * decay
    inner = jnp.einsum('clsh,cshp->clhp', scores, weighted, precision=HIGH)
    to_end = jnp.exp(cum[:, -1:, :] - cum)
    states = jnp.einsum('cshn,cshp->chpn', bb * to_end[..., None], weighted, precision=HIGH)
    totals = jnp.exp(cum[:, -1, :])

    def advance(carry, item):
        fresh, factor = item
        return (carry * factor[:, None, None] + fresh, carry)
    last, before = lax.scan(advance, init, (states, totals))
    outer = jnp.einsum('clhn,chpn->clhp', cc * jnp.exp(cum)[..., None], before, precision=HIGH)
    return ((inner + outer).reshape(length, heads, width), last)

def reference(residual, head_input, gate_input, b_input, c_input, step_input, conv_weight, conv_b_weight, conv_c_weight, step_bias, decay_log, skip, norm_gain, out_weight, ffn_gain, shared_gate, shared_up, shared_down, expert_gate, expert_up, expert_down, routes, route_weights):
    taps = jnp.concatenate([conv_weight, conv_b_weight, conv_c_weight], axis=1)
    rate = -jnp.exp(decay_log)
    per_group = HEADS // GROUPS
    span = GROUPS * STATE

    def one_sequence(items):
        x_seq, b_seq, c_seq, s_seq, g_seq, r_seq = items
        rows = jnp.concatenate([x_seq, b_seq, c_seq], axis=1)
        act = conv_silu(jnp.pad(rows, ((CONV_K - 1, 0), (0, 0))), taps, LENGTH)
        xs = act[:, :INNER].reshape(LENGTH, HEADS, HEAD_DIM)
        bm = jnp.repeat(act[:, INNER:INNER + span].reshape(LENGTH, GROUPS, STATE), per_group, axis=1)
        cm = jnp.repeat(act[:, INNER + span:].reshape(LENGTH, GROUPS, STATE), per_group, axis=1)
        step = jax.nn.softplus(s_seq.astype(jnp.float32) + step_bias[None, :])
        y, _ = block_scan(xs, step, rate, bm, cm, BLOCK, jnp.zeros((HEADS, HEAD_DIM, STATE), jnp.float32))
        scanned = (y + skip[None, :, None] * xs).reshape(LENGTH, INNER).astype(jnp.bfloat16)
        gated = (scanned.astype(jnp.float32) * jax.nn.silu(g_seq.astype(jnp.float32))).reshape(LENGTH, GROUPS, INNER // GROUPS)
        gated = gated * lax.rsqrt(lax.optimization_barrier(jnp.mean(gated * gated, axis=2, keepdims=True)) + EPS)
        normed = (gated.reshape(LENGTH, INNER) * norm_gain[None, :]).astype(jnp.bfloat16)
        mixed = (r_seq.astype(jnp.float32) + jnp.dot(normed, out_weight, preferred_element_type=jnp.float32)).astype(jnp.bfloat16)
        mixed_f = mixed.astype(jnp.float32)
        expert_in = (mixed_f * lax.rsqrt(lax.optimization_barrier(jnp.mean(mixed_f * mixed_f, axis=1, keepdims=True)) + EPS) * ffn_gain[None, :]).astype(jnp.bfloat16)
        shared_hidden = (jax.nn.silu(jnp.dot(expert_in, shared_gate, preferred_element_type=jnp.float32)) * jnp.dot(expert_in, shared_up, preferred_element_type=jnp.float32)).astype(jnp.bfloat16)
        base = mixed_f + jnp.dot(shared_hidden, shared_down, preferred_element_type=jnp.float32)
        return (base, expert_in)
    base, expert_in = lax.map(one_sequence, (head_input, b_input, c_input, step_input, gate_input, residual))
    rows_all = SEQS * LENGTH
    flat_in = expert_in.reshape(rows_all, D)
    chosen = routes.reshape(-1).astype(jnp.int32)
    pairs = chosen.shape[0]
    onehot = (chosen[:, None] == jnp.arange(EXPERTS, dtype=jnp.int32)[None, :]).astype(jnp.int32)
    rank = lax.optimization_barrier(jnp.sum((jnp.cumsum(onehot, axis=0) - onehot) * onehot, axis=1)).astype(jnp.int32)
    room = N_SP * N_DP * CAP
    table = jnp.full((EXPERTS, room), pairs, jnp.int32).at[chosen, rank].set(jnp.arange(pairs, dtype=jnp.int32))

    def serve(carry, item):
        index, gate_w, up_w, down_w = item
        rows = jnp.take(flat_in, jnp.minimum(index, pairs - 1) // TOP_K, axis=0)
        hidden = (jax.nn.silu(jnp.dot(rows, gate_w, preferred_element_type=jnp.float32)) * jnp.dot(rows, up_w, preferred_element_type=jnp.float32)).astype(jnp.bfloat16)
        done = jnp.dot(hidden, down_w, preferred_element_type=jnp.float32).astype(jnp.bfloat16)
        return (carry.at[index].set(done, mode='drop'), None)
    pair_out, _ = lax.scan(serve, jnp.zeros((pairs, D), jnp.bfloat16), (table, expert_gate, expert_up, expert_down))
    routed = lax.optimization_barrier(jnp.sum(pair_out.reshape(rows_all, TOP_K, D).astype(jnp.float32) * route_weights.reshape(rows_all, TOP_K, 1), axis=1))
    return (base.reshape(rows_all, D) + routed).astype(jnp.bfloat16).reshape(SEQS, LENGTH, D)
```

```python
import jax
import jax.numpy as jnp
from jax import lax
from jax.experimental import pallas as pl
from jax.experimental.pallas import tpu as pltpu
from jax.sharding import PartitionSpec as P

EPS = 1e-06
HIGH = lax.Precision.HIGHEST
HALO = 8
TAIL = 16
F32 = jnp.float32
BF16 = jnp.bfloat16
MESH = pl.DeviceIdType.MESH
CHUNKS = 4


def silu(v):
    return v * (1.0 / (1.0 + jnp.exp(-v)))


def conv_silu(halo, rows, taps):
    count = taps.shape[0]
    length = rows.shape[0]
    padded = jnp.concatenate([halo.astype(F32), rows.astype(F32)], axis=0)
    total = None
    for tap in range(count):
        start = HALO - (count - 1) + tap
        term = padded[start : start + length] * taps[tap : tap + 1].astype(F32)
        total = term if total is None else total + term
    return silu(total)


def spread(columns, first, count, width):
    rows = columns.shape[0]
    return jnp.concatenate(
        [jnp.broadcast_to(columns[:, first + j : first + j + 1], (rows, width)) for j in range(count)],
        axis=1,
    )


def block_kernel(
    x_ref, b_ref, c_ref, halo_ref, step_ref, wx_ref, wb_ref, wc_ref, bias_ref, log_ref, skip_ref,
    y_ref, cm_ref, grow_ref, state_ref, *, groups, local,
):
    length, inner = x_ref.shape
    heads = step_ref.shape[1]
    span = b_ref.shape[1]
    per = heads // groups
    width = inner // heads
    state = span // groups
    wide = per * width
    raw = step_ref[...].astype(F32) + bias_ref[...]
    step = jnp.maximum(raw, 0.0) + jnp.log(1.0 + jnp.exp(-jnp.abs(raw)))
    logs = step * -jnp.exp(log_ref[...])
    row = lax.broadcasted_iota(jnp.int32, (length, length), 0)
    col = lax.broadcasted_iota(jnp.int32, (length, length), 1)
    lower = row >= col
    tril = lower.astype(F32)
    cum = lax.dot_general(tril, logs, (((1,), (0,)), ((), ())), precision=HIGH, preferred_element_type=F32)
    cum_t = lax.dot_general(logs, tril, (((0,), (1,)), ((), ())), precision=HIGH, preferred_element_type=F32)
    grow_ref[...] = cum
    to_end = jnp.exp(cum[length - 1 : length] - cum)
    for g in range(groups):
        xcol = slice(g * wide, (g + 1) * wide)
        bcol = slice(g * state, (g + 1) * state)
        xs = conv_silu(halo_ref[:, xcol], x_ref[:, xcol], wx_ref[:, xcol])
        bm = conv_silu(
            halo_ref[:, inner + g * state : inner + (g + 1) * state], b_ref[:, bcol], wb_ref[:, bcol]
        ).astype(BF16)
        cm = conv_silu(
            halo_ref[:, inner + span + g * state : inner + span + (g + 1) * state],
            c_ref[:, bcol], wc_ref[:, bcol],
        ).astype(BF16)
        cm_ref[:, bcol] = cm
        weighted = xs * spread(step, g * per, per, width)
        scores = lax.dot_general(cm, bm, (((1,), (1,)), ((), ())), preferred_element_type=F32)
        scores = jnp.where(lower, scores, 0.0)
        parts = []
        small = weighted.astype(BF16)
        for j in range(per):
            h = g * per + j
            decay = jnp.exp(jnp.minimum(cum[:, h : h + 1] - cum_t[h : h + 1, :], 0.0))
            parts.append(
                jnp.dot((scores * decay).astype(BF16), small[:, j * width : (j + 1) * width],
                        preferred_element_type=F32)
            )
        y_ref[:, xcol] = jnp.concatenate(parts, axis=1) + skip_ref[:, xcol] * xs
        ended = (weighted * spread(to_end, g * per, per, width)).astype(BF16)
        fresh = lax.dot_general(
            ended, bm, (((0,), (0,)), ((), ())), preferred_element_type=F32
        ).astype(BF16)
        for j in range(per):
            h = g * per + j
            at = h % local * width
            state_ref[h // local, at : at + width, :] = fresh[j * width : (j + 1) * width]
    last = cum[length - 1 : length]
    high = last.astype(BF16)
    rest = last - high.astype(F32)
    middle = rest.astype(BF16)
    low = (rest - middle.astype(F32)).astype(BF16)
    for w in range(heads // local):
        mine = slice(w * local, (w + 1) * local)
        parts = [p.astype(F32)[:, mine] for p in (high, middle, low)]
        rows = jnp.concatenate(parts + [jnp.zeros((TAIL - 3, local), F32)], axis=0)
        rows = jnp.concatenate([rows, jnp.zeros((TAIL, state - local), F32)], axis=1)
        state_ref[w, local * width :, :] = rows.astype(BF16)


def prefix_kernel(got_ref, out_ref, *, local):
    ways, rows, state = out_ref.shape
    width = rows // local
    factors = []
    for i in range(ways - 1):
        tail = got_ref[i, rows : rows + TAIL, :].astype(F32)
        factors.append(jnp.exp(tail[0:1] + tail[1:2] + tail[2:3]))
    for j in range(local):
        at = slice(j * width, (j + 1) * width)
        carry = jnp.zeros((width, state), F32)
        for i in range(ways):
            out_ref[i, at, :] = carry.astype(BF16)
            if i < ways - 1:
                factor = jnp.broadcast_to(factors[i][:, j : j + 1], (1, state))
                carry = carry * factor + got_ref[i, at, :].astype(F32)


def norm_kernel(y_ref, cm_ref, grow_ref, before_ref, gate_ref, gain_ref, out_ref, *, groups):
    length, inner = y_ref.shape
    heads = grow_ref.shape[1]
    state = before_ref.shape[1]
    per = heads // groups
    width = inner // heads
    wide = per * width
    grow = jnp.exp(grow_ref[...])
    for g in range(groups):
        xcol = slice(g * wide, (g + 1) * wide)
        outer = lax.dot_general(
            cm_ref[:, g * state : (g + 1) * state], before_ref[xcol, :],
            (((1,), (1,)), ((), ())), preferred_element_type=F32,
        )
        v = y_ref[:, xcol] + outer * spread(grow, g * per, per, width)
        v = v * silu(gate_ref[:, xcol].astype(F32))
        v = v * lax.rsqrt(jnp.mean(v * v, axis=1, keepdims=True) + EPS)
        out_ref[:, xcol] = (v * gain_ref[:, xcol]).astype(BF16)


def pick(index, table):
    value = jnp.int32(table[0])
    for c in range(1, len(table)):
        value = jnp.where(index == c, jnp.int32(table[c]), value)
    return value


def layer_of_steps(depth):
    if depth == 4:
        mid, end = (1, 2), (0, 3)
        return [
            ("take", 1, None), ("take", 2, mid), ("give", 1, None), ("give", 2, mid), ("expert", 0, None),
            ("expert", 1, None), ("join", 0, None), ("take", 2, end), ("give", 2, end), ("take", 3, mid),
            ("give", 3, mid), ("join", 1, None), ("expert", 2, None), ("take", 3, end), ("give", 3, end),
            ("join", 2, None), ("expert", 3, None), ("join", 3, None),
        ]
    steps = [("expert", 0, None), ("join", 0, None)]
    for k in range(1, depth):
        steps += [("take", k, None), ("give", k, None), ("expert", k, None), ("join", k, None)]
    return steps


def moe_kernel(*refs, depth, side, ndp, picks, blocks):
    normed_ref, resid_ref, gain_ref, info_ref = refs[:4]
    w_ref = refs[4]
    shared_refs = refs[5:8]
    expert_refs = refs[8:11]
    out_ref = refs[11]
    (
        w_buf, sg_buf, su_buf, sd_buf, eg_buf, eu_buf, ed_buf, t_buf, info_buf, g_buf, x_buf, r_buf, p_buf, q_buf,
        acc, local_sem, info_send, info_recv, t_send, t_recv, g_send, x_recv, d_send, r_recv, c_send, q_recv,
    ) = refs[12:]
    tokens, model = t_buf.shape[1:]
    plane, slots = g_buf.shape[1:3]
    lanes = plane * slots
    rows = tokens // CHUNKS
    tile = min(512, model)
    sp, dp = lax.axis_index("sp"), lax.axis_index("dp")
    zi, me = sp // side, (sp % side) * ndp + dp
    order = [[z] + sorted((s for s in range(depth) if s != z), key=lambda s: (abs(s - z), s)) for z in range(depth)]
    source = [pick(zi, [order[z][k] for z in range(depth)]) for k in range(depth)]

    def peer(q):
        return (zi * side + q // ndp, q % ndp)

    def along(step):
        return (sp + step * side, dp)

    barrier = pltpu.get_barrier_semaphore()

    @pl.loop(1, plane)
    def _(j):
        pl.semaphore_signal(barrier, inc=1, device_id=peer((me + j) % plane), device_id_type=MESH)

    @pl.loop(1, depth)
    def _(j):
        pl.semaphore_signal(
            barrier, inc=1, device_id=((zi + j) % depth * side + sp % side, dp), device_id_type=MESH
        )

    w_rows = w_buf.shape[1]
    loads = []
    for i in range(blocks):
        loads.append(pltpu.make_async_copy(w_ref.at[pl.ds(i * w_rows, w_rows)], w_buf.at[i], local_sem.at[i]))
    for i, (a, b) in enumerate(zip(shared_refs, (sg_buf, su_buf, sd_buf))):
        loads.append(pltpu.make_async_copy(a, b, local_sem.at[blocks + i]))
    for i, (a, b) in enumerate(zip(expert_refs, (eg_buf, eu_buf, ed_buf))):
        loads.append(pltpu.make_async_copy(a.at[0], b, local_sem.at[blocks + 3 + i]))
    for c in loads:
        c.start()

    for i in range(blocks):
        loads[i].wait()
    square = jnp.zeros((tokens, 1), F32)
    for n in range(0, model, tile):
        cols = slice(n, n + tile)
        total = resid_ref[:, cols].astype(F32)
        for i in range(blocks):
            total = total + jnp.dot(
                normed_ref[:, i * w_rows : (i + 1) * w_rows], w_buf[i, :, cols], preferred_element_type=F32
            )
        total = total.astype(BF16).astype(F32)
        acc[:, cols] = total
        square = square + jnp.sum(total * total, axis=1, keepdims=True)
    scale = lax.rsqrt(square / model + EPS)
    for n in range(0, model, tile):
        cols = slice(n, n + tile)
        t_buf[zi, :, cols] = (acc[:, cols] * scale * gain_ref[:, cols]).astype(BF16)
    info_buf[zi] = info_ref[...]

    pl.semaphore_wait(barrier, plane - 1 + depth - 1)

    @pl.loop(1, depth)
    def _(j):
        pltpu.make_async_remote_copy(
            src_ref=info_ref, dst_ref=info_buf.at[zi], send_sem=info_send, recv_sem=info_recv.at[zi],
            device_id=((zi + j) % depth * side + sp % side, dp), device_id_type=MESH,
        ).start()

    def token_copy(s, j, up):
        part = pl.ds(j * rows, rows)
        return pltpu.make_async_remote_copy(
            src_ref=t_buf.at[s, part], dst_ref=t_buf.at[s, part], send_sem=t_send.at[1 if up else 0, s],
            recv_sem=t_recv.at[s, j], device_id=along(1 if up else -1), device_id_type=MESH,
        )

    def sum_copy(s, j, up):
        part = pl.ds(j * rows, rows)
        into = s if up else jnp.where(s == zi - 1, depth, s)
        return pltpu.make_async_remote_copy(
            src_ref=p_buf.at[s, part], dst_ref=q_buf.at[into, part], send_sem=c_send.at[s],
            recv_sem=q_recv.at[into, j], device_id=along(1 if up else -1), device_id_type=MESH,
        )

    def send_sum(s, j):
        @pl.when(s > zi)
        def _():
            sum_copy(s, j, True).start()

        @pl.when(s < zi)
        def _():
            sum_copy(s, j, False).start()

    def send_tokens(s, j):
        @pl.when((s <= zi) & (zi < depth - 1))
        def _():
            token_copy(s, j, True).start()

        @pl.when((s >= zi) & (zi > 0))
        def _():
            token_copy(s, j, False).start()

    def landed(ref, sem):
        pltpu.make_async_copy(ref, ref, sem).wait()

    def take(k):
        s = source[k]
        landed(info_buf.at[s], info_recv.at[s])
        for j in range(CHUNKS):
            landed(t_buf.at[s, pl.ds(j * rows, rows)], t_recv.at[s, j])
            send_tokens(s, j)

    def target():
        row = lax.broadcasted_iota(jnp.int32, (lanes, tokens), 0) + zi * lanes
        return row.astype(F32)

    def give(k):
        s = source[k]
        info = info_buf[s]
        slot = target()
        chosen = slot == info[0:1]
        for p in range(1, picks):
            chosen = chosen | (slot == info[p : p + 1])
        chosen = jnp.where(chosen, 1.0, 0.0).astype(BF16)
        for n in range(0, model, tile):
            cols = slice(n, n + tile)
            part = jnp.dot(chosen, t_buf[s, :, cols], preferred_element_type=F32).astype(BF16)
            g_buf[s, :, :, cols] = part.reshape(plane, slots, tile)

        @pl.loop(1, plane)
        def _(j):
            q = (me + j) % plane
            pltpu.make_async_remote_copy(
                src_ref=g_buf.at[s, q], dst_ref=x_buf.at[s, me], send_sem=g_send.at[s], recv_sem=x_recv.at[s],
                device_id=peer(q), device_id_type=MESH,
            ).start()

        x_buf[s, me] = g_buf[s, me]

    def expert(k):
        s = source[k]
        if k == 0:
            for c in loads[blocks + 3 :]:
                c.wait()
        landed(x_buf.at[s, pl.ds(0, plane - 1)], x_recv.at[s])
        rows_in = x_buf[s].reshape(lanes, model)
        gate = jnp.dot(rows_in, eg_buf[...], preferred_element_type=F32)
        up = jnp.dot(rows_in, eu_buf[...], preferred_element_type=F32)
        hidden = (silu(gate) * up).astype(BF16)
        for n in range(0, model, tile):
            cols = slice(n, n + tile)
            part = jnp.dot(hidden, ed_buf[:, cols], preferred_element_type=F32).astype(BF16)
            x_buf[s, :, :, cols] = part.reshape(plane, slots, tile)

        @pl.loop(1, plane)
        def _(j):
            q = (me + j) % plane
            pltpu.make_async_remote_copy(
                src_ref=x_buf.at[s, q], dst_ref=r_buf.at[s, me], send_sem=d_send.at[s], recv_sem=r_recv.at[s],
                device_id=peer(q), device_id_type=MESH,
            ).start()

        r_buf[s, me] = x_buf[s, me]

    def join(k):
        s = source[k]
        landed(r_buf.at[s, pl.ds(0, plane - 1)], r_recv.at[s])
        info = info_buf[s]
        slot = target()
        weight = jnp.zeros((lanes, tokens), F32)
        for p in range(picks):
            weight = weight + jnp.where(slot == info[p : p + 1], info[picks + p : picks + p + 1], 0.0)
        high = weight.astype(BF16)
        low = (weight - high.astype(F32)).astype(BF16)
        for n in range(0, model, tile):
            cols = slice(n, n + tile)
            block = r_buf[s, :, :, cols].reshape(lanes, tile)
            part = lax.dot_general(high, block, (((0,), (0,)), ((), ())), preferred_element_type=F32)
            part = part + lax.dot_general(low, block, (((0,), (0,)), ((), ())), preferred_element_type=F32)
            if k == 0:
                acc[:, cols] = acc[:, cols] + part
            else:
                p_buf[s, :, cols] = part.astype(BF16)
        if k:
            @pl.when((zi == 0) | (zi == depth - 1))
            def _():
                for j in range(CHUNKS):
                    send_sum(s, j)

    for j in range(CHUNKS):
        send_tokens(source[0], j)
    give(0)

    for c in loads[blocks : blocks + 3]:
        c.wait()
    x = t_buf[zi]
    hidden = silu(jnp.dot(x, sg_buf[...], preferred_element_type=F32)) * jnp.dot(
        x, su_buf[...], preferred_element_type=F32
    )
    hidden = hidden.astype(BF16)
    for n in range(0, model, tile):
        cols = slice(n, n + tile)
        acc[:, cols] = acc[:, cols] + jnp.dot(hidden, sd_buf[:, cols], preferred_element_type=F32)

    actions = {"take": take, "give": give, "expert": expert, "join": join}
    for name, k, planes in layer_of_steps(depth):
        if planes is None:
            actions[name](k)
        else:
            taken = zi == planes[0]
            for z in planes[1:]:
                taken = taken | (zi == z)

            @pl.when(taken)
            def _(name=name, k=k):
                actions[name](k)

    def far(z, s):
        return depth - 1 - s + depth - 1 - z if s < z else s + z

    passing = [sorted((s for s in range(depth) if s != z), key=lambda s, z=z: (far(z, s), s)) for z in range(depth)]

    @pl.when((zi > 0) & (zi < depth - 1))
    def _():
        for i in range(depth - 1):
            s = pick(zi, [passing[z][i] for z in range(depth)])
            for j in range(CHUNKS):
                part = pl.ds(j * rows, rows)
                landed(q_buf.at[s, part], q_recv.at[s, j])
                p_buf[s, part] = (p_buf[s, part].astype(F32) + q_buf[s, part].astype(F32)).astype(BF16)
                send_sum(s, j)

    for j in range(CHUNKS):
        part = pl.ds(j * rows, rows)

        @pl.when(zi > 0)
        def _():
            landed(q_buf.at[zi, part], q_recv.at[zi, j])
            acc[part] = acc[part] + q_buf[zi, part].astype(F32)

        @pl.when(zi < depth - 1)
        def _():
            landed(q_buf.at[depth, part], q_recv.at[depth, j])
            acc[part] = acc[part] + q_buf[depth, part].astype(F32)

        out_ref[part] = acc[part].astype(BF16)

    @pl.loop(1, depth)
    def _(j):
        landed(info_ref, info_send)

    for k in range(depth):
        s = source[k]
        landed(g_buf.at[s, pl.ds(0, plane - 1)], g_send.at[s])
        landed(x_buf.at[s, pl.ds(0, plane - 1)], d_send.at[s])
        if k:
            landed(p_buf.at[s], c_send.at[s])

        @pl.when((s <= zi) & (zi < depth - 1))
        def _():
            landed(t_buf.at[s], t_send.at[1, s])

        @pl.when((s >= zi) & (zi > 0))
        def _():
            landed(t_buf.at[s], t_send.at[0, s])


def vmem(count):
    return [pl.BlockSpec(memory_space=pltpu.VMEM)] * count


PARAMS = pltpu.CompilerParams(vmem_limit_bytes=32 * 1024 * 1024)


def body(
    residual, head_input, gate_input, b_input, c_input, step_input, conv_weight, conv_b_weight,
    conv_c_weight, step_bias, decay_log, skip, norm_gain, out_weight, ffn_gain, shared_gate,
    shared_up, shared_down, expert_gate, expert_up, expert_down, routes, route_weights,
):
    tokens, inner = head_input.shape[1:]
    heads = step_bias.shape[0]
    state = 128
    span = b_input.shape[2]
    groups = span // state
    width = inner // heads
    model = residual.shape[2]
    ways = lax.axis_size("sp")
    local = heads // ways
    x_rows, b_rows, c_rows = head_input[0], b_input[0], c_input[0]
    ndp = lax.axis_size("dp")
    weight = lax.all_gather(out_weight, "dp", axis=0, tiled=True)
    tail = jnp.concatenate([x_rows[-HALO:], b_rows[-HALO:], c_rows[-HALO:]], axis=1)
    halo = lax.ppermute(tail, "sp", [(i, i + 1) for i in range(ways - 1)])
    y, cm, cum, states = pl.pallas_call(
        lambda *refs: block_kernel(*refs, groups=groups, local=local),
        out_shape=(
            jax.ShapeDtypeStruct((tokens, inner), F32),
            jax.ShapeDtypeStruct((tokens, span), BF16),
            jax.ShapeDtypeStruct((tokens, heads), F32),
            jax.ShapeDtypeStruct((ways, local * width + TAIL, state), BF16),
        ),
        in_specs=vmem(11),
        out_specs=tuple(vmem(4)),
        compiler_params=PARAMS,
        cost_estimate=pl.CostEstimate(flops=400_000_000, bytes_accessed=5_000_000, transcendentals=1_500_000),
    )(
        x_rows, b_rows, c_rows, halo, step_input[0], conv_weight, conv_b_weight, conv_c_weight,
        step_bias[None], decay_log[None], jnp.repeat(skip, width)[None],
    )
    arrived = lax.all_to_all(states, "sp", split_axis=0, concat_axis=0, tiled=True)
    prefix = pl.pallas_call(
        lambda *refs: prefix_kernel(*refs, local=local),
        out_shape=jax.ShapeDtypeStruct((ways, local * width, state), BF16),
        in_specs=vmem(1),
        out_specs=vmem(1)[0],
        compiler_params=PARAMS,
        cost_estimate=pl.CostEstimate(flops=2_000_000, bytes_accessed=1_000_000, transcendentals=1000),
    )(arrived)
    before = lax.all_to_all(prefix, "sp", split_axis=0, concat_axis=0, tiled=True).reshape(inner, state)
    normed = pl.pallas_call(
        lambda *refs: norm_kernel(*refs, groups=groups),
        out_shape=jax.ShapeDtypeStruct((tokens, inner), BF16),
        in_specs=vmem(6),
        out_specs=vmem(1)[0],
        compiler_params=PARAMS,
        cost_estimate=pl.CostEstimate(flops=100_000_000, bytes_accessed=3_000_000, transcendentals=400_000),
    )(y, cm, cum, before, gate_input[0], norm_gain[None])

    picks = routes.shape[2]
    side = max(1, ndp // 2)
    depth = ways // side
    plane = side * ndp
    experts = ways * ndp
    slots = max(16, 2 * tokens * picks // experts)
    chosen = routes[0].reshape(-1)
    pairs = chosen.shape[0]
    onehot = (chosen[:, None] == jnp.arange(experts, dtype=jnp.int32)[None, :]).astype(BF16)
    earlier = (jnp.arange(pairs)[:, None] > jnp.arange(pairs)[None, :]).astype(BF16)
    counts = jnp.dot(earlier, onehot, preferred_element_type=F32)
    position = jnp.sum(counts * onehot.astype(F32), axis=1)
    place = (chosen.astype(F32) * slots + position).reshape(tokens, picks)
    info = jnp.concatenate([place.T, route_weights[0].T, jnp.zeros((8 - 2 * picks, tokens), F32)], axis=0)

    hbm = [pl.BlockSpec(memory_space=pl.ANY)]
    dma = pltpu.SemaphoreType.DMA
    hidden = expert_gate.shape[2]
    shared = shared_gate.shape[1]
    out = pl.pallas_call(
        lambda *refs: moe_kernel(*refs, depth=depth, side=side, ndp=ndp, picks=picks, blocks=ndp),
        out_shape=jax.ShapeDtypeStruct((tokens, model), BF16),
        in_specs=vmem(4) + hbm * 7,
        out_specs=vmem(1)[0],
        scratch_shapes=[
            pltpu.VMEM((ndp, inner // ndp, model), BF16),
            pltpu.VMEM((model, shared), BF16),
            pltpu.VMEM((model, shared), BF16),
            pltpu.VMEM((shared, model), BF16),
            pltpu.VMEM((model, hidden), BF16),
            pltpu.VMEM((model, hidden), BF16),
            pltpu.VMEM((hidden, model), BF16),
            pltpu.VMEM((depth, tokens, model), BF16),
            pltpu.VMEM((depth, 8, tokens), F32),
            pltpu.VMEM((depth, plane, slots, model), BF16),
            pltpu.VMEM((depth, plane, slots, model), BF16),
            pltpu.VMEM((depth, plane, slots, model), BF16),
            pltpu.VMEM((depth, tokens, model), BF16),
            pltpu.VMEM((depth + 1, tokens, model), BF16),
            pltpu.VMEM((tokens, model), F32),
            dma((ndp + 6,)),
            dma, dma((depth,)), dma((2, depth)), dma((depth, CHUNKS)), dma((depth,)), dma((depth,)),
            dma((depth,)), dma((depth,)), dma((depth,)), dma((depth + 1, CHUNKS)),
        ],
        compiler_params=pltpu.CompilerParams(
            vmem_limit_bytes=61 * 1024 * 1024, collective_id=1, has_side_effects=True
        ),
        cost_estimate=pl.CostEstimate(flops=8_000_000_000, bytes_accessed=24_000_000, transcendentals=500_000),
    )(
        normed, residual[0], ffn_gain[None], info, weight, shared_gate, shared_up, shared_down,
        expert_gate, expert_up, expert_down,
    )
    return out[None]


def solution(mesh):
    rows = P("dp", "sp", None)
    split = P(("sp", "dp"), None, None)
    return jax.shard_map(
        body,
        mesh=mesh,
        in_specs=(rows,) * 6 + (P(),) * 7 + (P("dp", None),) + (P(),) * 4 + (split,) * 3 + (rows,) * 2,
        out_specs=rows,
        check_vma=False,
    )
```

```python
import jax
import jax.numpy as jnp
from jax import lax
from jax.experimental import pallas as pl
from jax.experimental.pallas import tpu as pltpu
from jax.sharding import PartitionSpec as P

EPS = 1e-06
HIGH = lax.Precision.HIGHEST
HALO = 8
TAIL = 16
PACK = 128
F32 = jnp.float32
BF16 = jnp.bfloat16
MESH = pl.DeviceIdType.MESH
CHUNKS = 4
PARTS = 4


def silu(v):
    return v * (1.0 / (1.0 + jnp.exp(-v)))


def conv_silu(halo, rows, taps):
    count = taps.shape[0]
    length = rows.shape[0]
    padded = jnp.concatenate([halo.astype(F32)[-HALO:], rows.astype(F32)], axis=0)
    total = None
    for tap in range(count):
        start = HALO - (count - 1) + tap
        term = padded[start : start + length] * taps[tap : tap + 1].astype(F32)
        total = term if total is None else total + term
    return silu(total)


def spread(columns, first, count, width):
    rows = columns.shape[0]
    return jnp.concatenate(
        [jnp.broadcast_to(columns[:, first + j : first + j + 1], (rows, width)) for j in range(count)],
        axis=1,
    )


def pick(index, table):
    value = jnp.int32(table[0])
    for c in range(1, len(table)):
        value = jnp.where(index == c, jnp.int32(table[c]), value)
    return value


def layer_of_steps(depth):
    if depth == 4:
        mid, end = (1, 2), (0, 3)
        return [
            ("take", 1, None), ("take", 2, mid), ("give", 1, None), ("give", 2, mid), ("expert", 0, None),
            ("expert", 1, None), ("join", 0, None), ("take", 2, end), ("give", 2, end), ("take", 3, mid),
            ("give", 3, mid), ("join", 1, None), ("expert", 2, None), ("take", 3, end), ("give", 3, end),
            ("join", 2, None), ("expert", 3, None), ("join", 3, None),
        ]
    steps = [("expert", 0, None), ("join", 0, None)]
    for k in range(1, depth):
        steps += [("take", k, None), ("give", k, None), ("expert", k, None), ("join", k, None)]
    return steps


def layer_kernel(
    step_ref, route_ref, share_ref, bias_ref, log_ref, skip_ref, x_ref, b_ref, c_ref, gate_ref, resid_ref, wx_ref, wb_ref, wc_ref, ngain_ref, fgain_ref, w_ref,
    sg_ref, su_ref, sd_ref, eg_ref, eu_ref, ed_ref, out_ref,
    step_in, route_in, share_in, bias_in, log_in, skip_in, xin, bin_, cin, gin, rin, wx, wb, wc, ngain, fgain, w_buf, sg_buf, su_buf, sd_buf, eg_buf, eu_buf, ed_buf,
    xh, bh, ch, y_buf, cm_buf, cum_buf, own_last, last_buf, st_buf, f_buf, b_buf, o_buf, c_buf, bef_buf, normed,
    t_buf, info, info_buf, g_buf, x_buf, r_buf, p_buf, q_buf, acc,
    local_sem, h_send, h_recv, l_send, l_recv, f_send, f_recv, b_send, b_recv, o_send, o_recv,
    w_send, w_pass, w_recv, info_send, info_recv, t_send, t_recv, g_send, x_recv, d_send, r_recv, c_send, q_recv,
    *, depth, side, ndp, ways, picks, experts, heads,
):
    tokens, model = t_buf.shape[1:]
    plane, slots = g_buf.shape[1:3]
    groups, wide, state = st_buf.shape
    inner = groups * wide
    per = heads // groups
    width = inner // heads
    share = groups // side
    lanes = plane * slots
    rows = tokens // CHUNKS
    tile = min(512, model)
    sp, dp = lax.axis_index("sp"), lax.axis_index("dp")
    zi, yi = sp // side, sp % side
    me = yi * ndp + dp
    mate = dp + 1 - 2 * (dp % 2)
    order = [[z] + sorted((s for s in range(depth) if s != z), key=lambda s: (abs(s - z), s)) for z in range(depth)]
    source = [pick(zi, [order[z][k] for z in range(depth)]) for k in range(depth)]

    def peer(q):
        return (zi * side + q // ndp, q % ndp)

    def along(step):
        return (sp + step * side, dp)

    def landed(ref, sem):
        pltpu.make_async_copy(ref, ref, sem).wait()

    def remote(src, dst, send, recv, device):
        pltpu.make_async_remote_copy(
            src_ref=src, dst_ref=dst, send_sem=send, recv_sem=recv, device_id=device, device_id_type=MESH
        ).start()

    local = [
        (x_ref, xin), (b_ref, bin_), (c_ref, cin), (wx_ref, wx), (wb_ref, wb), (wc_ref, wc),
        (step_ref, step_in), (route_ref, route_in), (share_ref, share_in), (bias_ref, bias_in), (log_ref, log_in),
        (skip_ref, skip_in),
        (gate_ref, gin), (ngain_ref, ngain), (w_ref, w_buf.at[dp]), (resid_ref, rin), (fgain_ref, fgain),
        (sg_ref, sg_buf), (su_ref, su_buf), (sd_ref, sd_buf),
        (eg_ref.at[0], eg_buf), (eu_ref.at[0], eu_buf), (ed_ref.at[0], ed_buf),
    ]
    loads = [pltpu.make_async_copy(a, b, local_sem.at[i]) for i, (a, b) in enumerate(local)]
    for c in loads:
        c.start()

    barrier = pltpu.get_barrier_semaphore()

    @pl.loop(1, plane)
    def _(j):
        pl.semaphore_signal(barrier, inc=1, device_id=peer((me + j) % plane), device_id_type=MESH)

    @pl.loop(1, depth)
    def _(j):
        pl.semaphore_signal(
            barrier, inc=1, device_id=((zi + j) % depth * side + sp % side, dp), device_id_type=MESH
        )

    for step in (1, ways - 1):
        pl.semaphore_signal(barrier, inc=1, device_id=((sp + step) % ways, dp), device_id_type=MESH)
    pl.semaphore_wait(barrier, plane - 1 + depth - 1 + 2)

    w_rows = w_buf.shape[1]
    piece = w_rows // PARTS
    for hop in range(2, ndp, 2):
        for j in range(PARTS):
            part = pl.ds(j * piece, piece)
            remote(w_ref.at[part], w_buf.at[dp, part], w_send.at[hop // 2], w_recv.at[dp, j], (sp, (dp + hop) % ndp))
    for j in range(PARTS):
        part = pl.ds(j * piece, piece)
        remote(w_ref.at[part], w_buf.at[dp, part], w_send.at[0], w_recv.at[dp, j], (sp, mate))

    for i in range(3):
        loads[i].wait()
    edge = pl.ds(tokens - TAIL, TAIL)

    @pl.when(sp < ways - 1)
    def _():
        for i, (a, b) in enumerate(((xin, xh), (bin_, bh), (cin, ch))):
            remote(a.at[edge], b, h_send.at[i], h_recv.at[i], (sp + 1, dp))

    for i in range(6, 12):
        loads[i].wait()
    raw = step_in[...].astype(F32).T + bias_in[...]
    rate = -jnp.exp(log_in[...])
    skip = skip_in[...]
    step = jnp.maximum(raw, 0.0) + jnp.log(1.0 + jnp.exp(-jnp.abs(raw)))
    logs = step * rate
    row = lax.broadcasted_iota(jnp.int32, (tokens, tokens), 0)
    col = lax.broadcasted_iota(jnp.int32, (tokens, tokens), 1)
    lower = row >= col
    tril = lower.astype(F32)
    cum = lax.dot_general(tril, logs, (((1,), (0,)), ((), ())), precision=HIGH, preferred_element_type=F32)
    cum_t = lax.dot_general(logs, tril, (((0,), (1,)), ((), ())), precision=HIGH, preferred_element_type=F32)
    cum_buf[...] = cum
    last = cum[tokens - 1 : tokens]
    padded = jnp.concatenate([last, jnp.zeros((1, PACK - heads), F32)], axis=1)
    padded = jnp.broadcast_to(padded, (8, PACK))
    own_last[...] = padded
    last_buf[yi] = padded
    to_end = jnp.exp(last - cum)

    @pl.loop(1, side)
    def _(o):
        to = (yi + o) % side
        remote(own_last, last_buf.at[yi], l_send, l_recv.at[yi], (zi * side + to, dp))

    before = jnp.where(row < col, 1.0, 0.0).astype(BF16)
    label = lax.broadcasted_iota(jnp.int32, (experts, tokens), 0).astype(F32)
    lines, used = [], jnp.zeros((experts, 1), F32)
    for p in range(picks):
        named = route_in[p : p + 1].astype(F32)
        hot = jnp.where(label == named, 1.0, 0.0)
        ahead = jnp.dot(hot.astype(BF16), before, preferred_element_type=F32) + used
        used = used + jnp.sum(hot, axis=1, keepdims=True)
        lines.append(named * slots + jnp.sum(ahead * hot, axis=0, keepdims=True))
    lines += [share_in[...], jnp.zeros((8 - 2 * picks, tokens), F32)]
    listed = jnp.concatenate(lines, axis=0)
    info[...] = listed
    info_buf[zi] = listed

    @pl.loop(1, depth)
    def _(j):
        remote(info, info_buf.at[zi], info_send, info_recv.at[zi], ((zi + j) % depth * side + yi, dp))

    for c in loads[3:6]:
        c.wait()

    @pl.when(sp == 0)
    def _():
        for h in (xh, bh, ch):
            h[...] = jnp.zeros(h.shape, BF16)

    @pl.when(sp > 0)
    def _():
        for i, h in enumerate((xh, bh, ch)):
            landed(h, h_recv.at[i])

    turns = [o * share + gl for gl in range(share) for o in range(side)]
    for g in turns:
        xcol = slice(g * wide, (g + 1) * wide)
        bcol = slice(g * state, (g + 1) * state)
        xs = conv_silu(xh[:, xcol], xin[:, xcol], wx[:, xcol])
        bm = conv_silu(bh[:, bcol], bin_[:, bcol], wb[:, bcol]).astype(BF16)
        cm = conv_silu(ch[:, bcol], cin[:, bcol], wc[:, bcol]).astype(BF16)
        cm_buf[:, bcol] = cm
        weighted = xs * spread(step, g * per, per, width)
        ended = (weighted * spread(to_end, g * per, per, width)).astype(BF16)
        fresh = lax.dot_general(ended, bm, (((0,), (0,)), ((), ())), preferred_element_type=F32).astype(BF16)
        st_buf[g] = fresh
        owner, gl = g // share, g % share

        @pl.when(owner != yi)
        def _():
            remote(
                st_buf.at[g], f_buf.at[yi, gl], f_send.at[gl], f_recv.at[yi, gl], (zi * side + owner, dp)
            )

        @pl.when(owner == yi)
        def _():
            f_buf[yi, gl] = fresh

        scores = lax.dot_general(cm, bm, (((1,), (1,)), ((), ())), preferred_element_type=F32)
        scores = jnp.where(lower, scores, 0.0)
        parts = []
        small = weighted.astype(BF16)
        for j in range(per):
            h = g * per + j
            decay = jnp.exp(jnp.minimum(cum[:, h : h + 1] - cum_t[h : h + 1, :], 0.0))
            parts.append(
                jnp.dot((scores * decay).astype(BF16), small[:, j * width : (j + 1) * width],
                        preferred_element_type=F32)
            )
        y_buf[:, xcol] = jnp.concatenate(parts, axis=1) + spread(skip, g * per, per, width) * xs

    @pl.loop(1, side)
    def _(o):
        landed(last_buf.at[(yi + o) % side], l_recv.at[(yi + o) % side])

    head = lax.broadcasted_iota(jnp.int32, (wide, PACK), 0) // width
    lane = lax.broadcasted_iota(jnp.int32, (wide, PACK), 1)
    held = [jnp.exp(last_buf[o, 0:1]) for o in range(side)]
    for gl in range(share):
        g = yi * share + gl
        mine = lane == head + g * per
        factors = [jnp.sum(jnp.where(mine, held[o], 0.0), axis=1, keepdims=True) for o in range(side)]
        for o in range(1, side):
            other = (yi + o) % side
            landed(f_buf.at[other, gl], f_recv.at[other, gl])

        @pl.when(zi == 0)
        def _():
            b_buf[gl] = jnp.zeros((wide, state), BF16)

        @pl.when(zi > 0)
        def _():
            landed(b_buf.at[gl], b_recv.at[gl])

        carry = b_buf[gl].astype(F32)
        for o in range(side):
            o_buf[o, gl] = carry.astype(BF16)
            carry = carry * factors[o] + f_buf[o, gl].astype(F32)
        c_buf[gl] = carry.astype(BF16)

        @pl.when(zi < depth - 1)
        def _():
            remote(c_buf.at[gl], b_buf.at[gl], b_send.at[gl], b_recv.at[gl], along(1))

        for o in range(1, side):
            other = (yi + o) % side
            remote(
                o_buf.at[other, gl], bef_buf.at[g], o_send.at[gl], o_recv.at[g], (zi * side + other, dp)
            )
        bef_buf[g] = o_buf[yi, gl]

    for i in (12, 13):
        loads[i].wait()
    grow = jnp.exp(cum_buf[...])
    for g in turns:
        xcol = slice(g * wide, (g + 1) * wide)

        @pl.when(g // share != yi)
        def _():
            landed(bef_buf.at[g], o_recv.at[g])

        outer = lax.dot_general(
            cm_buf[:, g * state : (g + 1) * state], bef_buf[g], (((1,), (1,)), ((), ())), preferred_element_type=F32
        )
        v = y_buf[:, xcol] + outer * spread(grow, g * per, per, width)
        v = v * silu(gin[:, xcol].astype(F32))
        v = v * lax.rsqrt(jnp.mean(v * v, axis=1, keepdims=True) + EPS)
        normed[:, xcol] = (v * ngain[:, xcol]).astype(BF16)

    for i in range(14, 17):
        loads[i].wait()
    for hop in range(2, ndp, 2):
        held_by = (dp + ndp - hop) % ndp
        for j in range(PARTS):
            part = pl.ds(j * piece, piece)
            landed(w_buf.at[held_by, part], w_recv.at[held_by, j])
            remote(
                w_buf.at[held_by, part], w_buf.at[held_by, part], w_pass.at[hop // 2], w_recv.at[held_by, j], (sp, mate)
            )
    for hop in range(0, ndp, 2):
        held_by = (mate + ndp - hop) % ndp
        for j in range(PARTS):
            landed(w_buf.at[held_by, pl.ds(j * piece, piece)], w_recv.at[held_by, j])
    square = jnp.zeros((tokens, 1), F32)
    for n in range(0, model, tile):
        cols = slice(n, n + tile)
        total = rin[:, cols].astype(F32)
        for i in range(ndp):
            total = total + jnp.dot(
                normed[:, i * w_rows : (i + 1) * w_rows], w_buf[i, :, cols], preferred_element_type=F32
            )
        total = total.astype(BF16).astype(F32)
        acc[:, cols] = total
        square = square + jnp.sum(total * total, axis=1, keepdims=True)
    scale = lax.rsqrt(square / model + EPS)
    for n in range(0, model, tile):
        cols = slice(n, n + tile)
        t_buf[zi, :, cols] = (acc[:, cols] * scale * fgain[:, cols]).astype(BF16)

    def token_copy(s, j, up):
        part = pl.ds(j * rows, rows)
        return pltpu.make_async_remote_copy(
            src_ref=t_buf.at[s, part], dst_ref=t_buf.at[s, part], send_sem=t_send.at[1 if up else 0, s],
            recv_sem=t_recv.at[s, j], device_id=along(1 if up else -1), device_id_type=MESH,
        )

    def sum_copy(s, j, up):
        part = pl.ds(j * rows, rows)
        into = s if up else jnp.where(s == zi - 1, depth, s)
        return pltpu.make_async_remote_copy(
            src_ref=p_buf.at[s, part], dst_ref=q_buf.at[into, part], send_sem=c_send.at[s],
            recv_sem=q_recv.at[into, j], device_id=along(1 if up else -1), device_id_type=MESH,
        )

    def send_sum(s, j):
        @pl.when(s > zi)
        def _():
            sum_copy(s, j, True).start()

        @pl.when(s < zi)
        def _():
            sum_copy(s, j, False).start()

    def send_tokens(s, j):
        @pl.when((s <= zi) & (zi < depth - 1))
        def _():
            token_copy(s, j, True).start()

        @pl.when((s >= zi) & (zi > 0))
        def _():
            token_copy(s, j, False).start()

    def take(k):
        s = source[k]
        landed(info_buf.at[s], info_recv.at[s])
        for j in range(CHUNKS):
            landed(t_buf.at[s, pl.ds(j * rows, rows)], t_recv.at[s, j])
            send_tokens(s, j)

    def target():
        row = lax.broadcasted_iota(jnp.int32, (lanes, tokens), 0) + zi * lanes
        return row.astype(F32)

    def give(k):
        s = source[k]
        listing = info_buf[s]
        slot = target()
        chosen = slot == listing[0:1]
        for p in range(1, picks):
            chosen = chosen | (slot == listing[p : p + 1])
        chosen = jnp.where(chosen, 1.0, 0.0).astype(BF16)
        for n in range(0, model, tile):
            cols = slice(n, n + tile)
            part = jnp.dot(chosen, t_buf[s, :, cols], preferred_element_type=F32).astype(BF16)
            g_buf[s, :, :, cols] = part.reshape(plane, slots, tile)

        @pl.loop(1, plane)
        def _(j):
            q = (me + j) % plane
            pltpu.make_async_remote_copy(
                src_ref=g_buf.at[s, q], dst_ref=x_buf.at[s, me], send_sem=g_send.at[s], recv_sem=x_recv.at[s],
                device_id=peer(q), device_id_type=MESH,
            ).start()

        x_buf[s, me] = g_buf[s, me]

    def expert(k):
        s = source[k]
        if k == 0:
            for c in loads[20:]:
                c.wait()
        landed(x_buf.at[s, pl.ds(0, plane - 1)], x_recv.at[s])
        rows_in = x_buf[s].reshape(lanes, model)
        gate = jnp.dot(rows_in, eg_buf[...], preferred_element_type=F32)
        up = jnp.dot(rows_in, eu_buf[...], preferred_element_type=F32)
        hidden = (silu(gate) * up).astype(BF16)
        for n in range(0, model, tile):
            cols = slice(n, n + tile)
            part = jnp.dot(hidden, ed_buf[:, cols], preferred_element_type=F32).astype(BF16)
            x_buf[s, :, :, cols] = part.reshape(plane, slots, tile)

        @pl.loop(1, plane)
        def _(j):
            q = (me + j) % plane
            pltpu.make_async_remote_copy(
                src_ref=x_buf.at[s, q], dst_ref=r_buf.at[s, me], send_sem=d_send.at[s], recv_sem=r_recv.at[s],
                device_id=peer(q), device_id_type=MESH,
            ).start()

        r_buf[s, me] = x_buf[s, me]

    def join(k):
        s = source[k]
        landed(r_buf.at[s, pl.ds(0, plane - 1)], r_recv.at[s])
        listing = info_buf[s]
        slot = target()
        weight = jnp.zeros((lanes, tokens), F32)
        for p in range(picks):
            weight = weight + jnp.where(slot == listing[p : p + 1], listing[picks + p : picks + p + 1], 0.0)
        high = weight.astype(BF16)
        low = (weight - high.astype(F32)).astype(BF16)
        for n in range(0, model, tile):
            cols = slice(n, n + tile)
            block = r_buf[s, :, :, cols].reshape(lanes, tile)
            part = lax.dot_general(high, block, (((0,), (0,)), ((), ())), preferred_element_type=F32)
            part = part + lax.dot_general(low, block, (((0,), (0,)), ((), ())), preferred_element_type=F32)
            if k == 0:
                acc[:, cols] = acc[:, cols] + part
            else:
                p_buf[s, :, cols] = part.astype(BF16)
        if k:
            @pl.when((zi == 0) | (zi == depth - 1))
            def _():
                for j in range(CHUNKS):
                    send_sum(s, j)

    for j in range(CHUNKS):
        send_tokens(source[0], j)
    give(0)

    for c in loads[17:20]:
        c.wait()
    x = t_buf[zi]
    hidden = silu(jnp.dot(x, sg_buf[...], preferred_element_type=F32)) * jnp.dot(
        x, su_buf[...], preferred_element_type=F32
    )
    hidden = hidden.astype(BF16)
    for n in range(0, model, tile):
        cols = slice(n, n + tile)
        acc[:, cols] = acc[:, cols] + jnp.dot(hidden, sd_buf[:, cols], preferred_element_type=F32)

    actions = {"take": take, "give": give, "expert": expert, "join": join}
    for name, k, planes in layer_of_steps(depth):
        if planes is None:
            actions[name](k)
        else:
            taken = zi == planes[0]
            for z in planes[1:]:
                taken = taken | (zi == z)

            @pl.when(taken)
            def _(name=name, k=k):
                actions[name](k)

    def far(z, s):
        return depth - 1 - s + depth - 1 - z if s < z else s + z

    passing = [sorted((s for s in range(depth) if s != z), key=lambda s, z=z: (far(z, s), s)) for z in range(depth)]

    @pl.when((zi > 0) & (zi < depth - 1))
    def _():
        for i in range(depth - 1):
            s = pick(zi, [passing[z][i] for z in range(depth)])
            for j in range(CHUNKS):
                part = pl.ds(j * rows, rows)
                landed(q_buf.at[s, part], q_recv.at[s, j])
                p_buf[s, part] = (p_buf[s, part].astype(F32) + q_buf[s, part].astype(F32)).astype(BF16)
                send_sum(s, j)

    for j in range(CHUNKS):
        part = pl.ds(j * rows, rows)

        @pl.when(zi > 0)
        def _():
            landed(q_buf.at[zi, part], q_recv.at[zi, j])
            acc[part] = acc[part] + q_buf[zi, part].astype(F32)

        @pl.when(zi < depth - 1)
        def _():
            landed(q_buf.at[depth, part], q_recv.at[depth, j])
            acc[part] = acc[part] + q_buf[depth, part].astype(F32)

        out_ref[part] = acc[part].astype(BF16)

    @pl.loop(1, depth)
    def _(j):
        landed(info, info_send)

    @pl.loop(1, side)
    def _(o):
        landed(own_last, l_send)

    @pl.when(sp < ways - 1)
    def _():
        for i, h in enumerate((xh, bh, ch)):
            landed(h, h_send.at[i])

    for gl in range(share):
        for _ in range(1, side):
            landed(st_buf.at[0], f_send.at[gl])
            landed(st_buf.at[0], o_send.at[gl])

        @pl.when(zi < depth - 1)
        def _():
            landed(c_buf.at[gl], b_send.at[gl])

    for hop in range(0, ndp, 2):
        landed(w_buf.at[0], w_send.at[hop // 2])
        if hop:
            landed(w_buf.at[0], w_pass.at[hop // 2])

    for k in range(depth):
        s = source[k]
        landed(g_buf.at[s, pl.ds(0, plane - 1)], g_send.at[s])
        landed(x_buf.at[s, pl.ds(0, plane - 1)], d_send.at[s])
        if k:
            landed(p_buf.at[s], c_send.at[s])

        @pl.when((s <= zi) & (zi < depth - 1))
        def _():
            landed(t_buf.at[s], t_send.at[1, s])

        @pl.when((s >= zi) & (zi > 0))
        def _():
            landed(t_buf.at[s], t_send.at[0, s])


def vmem(count):
    return [pl.BlockSpec(memory_space=pltpu.VMEM)] * count


def body(
    residual, head_input, gate_input, b_input, c_input, step_input, conv_weight, conv_b_weight,
    conv_c_weight, step_bias, decay_log, skip, norm_gain, out_weight, ffn_gain, shared_gate,
    shared_up, shared_down, expert_gate, expert_up, expert_down, routes, route_weights,
):
    tokens, inner = head_input.shape[1:]
    heads = step_bias.shape[0]
    state = 128
    span = b_input.shape[2]
    groups = span // state
    model = residual.shape[2]
    ways, ndp = lax.axis_size("sp"), lax.axis_size("dp")
    picks = routes.shape[2]
    side = max(1, ndp // 2)
    depth = ways // side
    plane = side * ndp
    experts = ways * ndp
    slots = max(16, 2 * tokens * picks // experts)
    share = groups // side
    wide = inner // groups
    hbm = [pl.BlockSpec(memory_space=pl.ANY)]
    dma = pltpu.SemaphoreType.DMA
    hidden = expert_gate.shape[2]
    shared = shared_gate.shape[1]

    def halves(*shape):
        return pltpu.VMEM(shape, BF16)

    def floats(*shape):
        return pltpu.VMEM(shape, F32)

    out = pl.pallas_call(
        lambda *refs: layer_kernel(
            *refs, depth=depth, side=side, ndp=ndp, ways=ways, picks=picks, experts=experts, heads=heads
        ),
        out_shape=jax.ShapeDtypeStruct((tokens, model), BF16),
        in_specs=hbm * 23,
        out_specs=vmem(1)[0],
        scratch_shapes=[
            halves(heads, tokens), pltpu.VMEM((picks, tokens), jnp.int32), floats(picks, tokens), floats(1, heads),
            floats(1, heads), floats(1, heads), halves(tokens, inner), halves(tokens, span), halves(tokens, span),
            halves(tokens, inner), halves(tokens, model), halves(*conv_weight.shape), halves(*conv_b_weight.shape),
            halves(*conv_c_weight.shape), floats(1, inner), floats(1, model),
            halves(ndp, inner // ndp, model), halves(model, shared), halves(model, shared), halves(shared, model),
            halves(model, hidden), halves(model, hidden), halves(hidden, model),
            halves(TAIL, inner), halves(TAIL, span), halves(TAIL, span), floats(tokens, inner), halves(tokens, span),
            floats(tokens, heads), floats(8, PACK), floats(side, 8, PACK), halves(groups, wide, state),
            halves(side, share, wide, state), halves(share, wide, state), halves(side, share, wide, state),
            halves(share, wide, state), halves(groups, wide, state), halves(tokens, inner),
            halves(depth, tokens, model), floats(8, tokens), floats(depth, 8, tokens),
            halves(depth, plane, slots, model), halves(depth, plane, slots, model), halves(depth, plane, slots, model),
            halves(depth, tokens, model), halves(depth + 1, tokens, model), floats(tokens, model),
            dma((23,)), dma((3,)), dma((3,)), dma, dma((side,)), dma((share,)), dma((side, share)), dma((share,)),
            dma((share,)), dma((share,)), dma((groups,)), dma((max(1, ndp // 2),)), dma((max(1, ndp // 2),)),
            dma((ndp, PARTS)),
            dma, dma((depth,)), dma((2, depth)), dma((depth, CHUNKS)), dma((depth,)), dma((depth,)),
            dma((depth,)), dma((depth,)), dma((depth,)), dma((depth + 1, CHUNKS)),
        ],
        compiler_params=pltpu.CompilerParams(
            vmem_limit_bytes=63 * 1024 * 1024, collective_id=1, has_side_effects=True
        ),
        cost_estimate=pl.CostEstimate(flops=8_000_000_000, bytes_accessed=24_000_000, transcendentals=500_000),
    )(
        step_input[0].T, routes[0].T, route_weights[0].T, step_bias[None], decay_log[None], skip[None], head_input[0], b_input[0], c_input[0], gate_input[0], residual[0], conv_weight, conv_b_weight,
        conv_c_weight, norm_gain[None], ffn_gain[None], out_weight, shared_gate, shared_up, shared_down,
        expert_gate, expert_up, expert_down,
    )
    return out[None]


def solution(mesh):
    rows = P("dp", "sp", None)
    split = P(("sp", "dp"), None, None)
    return jax.shard_map(
        body,
        mesh=mesh,
        in_specs=(rows,) * 6 + (P(),) * 7 + (P("dp", None),) + (P(),) * 4 + (split,) * 3 + (rows,) * 2,
        out_specs=rows,
        check_vma=False,
    )
```

```python
import jax
import jax.numpy as jnp
from jax import lax
from jax.experimental import pallas as pl
from jax.experimental.pallas import tpu as pltpu
from jax.sharding import PartitionSpec as P

EPS = 1e-06
HIGH = lax.Precision.HIGHEST
HALO = 8
TAIL = 16
PACK = 128
F32 = jnp.float32
BF16 = jnp.bfloat16
MESH = pl.DeviceIdType.MESH
CHUNKS = 8
PARTS = 16


def silu(v):
    return v * (1.0 / (1.0 + jnp.exp(-v)))


def conv_silu(halo, rows, taps):
    count = taps.shape[0]
    length = rows.shape[0]
    padded = jnp.concatenate([halo.astype(F32)[-HALO:], rows.astype(F32)], axis=0)
    total = None
    for tap in range(count):
        start = HALO - (count - 1) + tap
        term = padded[start : start + length] * taps[tap : tap + 1].astype(F32)
        total = term if total is None else total + term
    return silu(total)


def spread(columns, first, count, width):
    rows = columns.shape[0]
    return jnp.concatenate(
        [jnp.broadcast_to(columns[:, first + j : first + j + 1], (rows, width)) for j in range(count)],
        axis=1,
    )


def pick(index, table):
    value = jnp.int32(table[0])
    for c in range(1, len(table)):
        value = jnp.where(index == c, jnp.int32(table[c]), value)
    return value


def orders(depth):
    if depth == 4:
        return [[0, 1, 3, 2], [1, 0, 2, 3], [2, 3, 1, 0], [3, 2, 0, 1]]
    return [[z] + sorted((s for s in range(depth) if s != z), key=lambda s: (abs(s - z), s)) for z in range(depth)]


def layer_of_steps(depth):
    if depth == 4:
        mid, end = (1, 2), (0, 3)
        return [
            ("expert", 0, None), ("take", 1, end), ("pair", 1, mid), ("give", 1, None),
            ("give", 2, mid), ("join", 0, end), ("take", 3, mid), ("late", 2, mid), ("expert", 1, None),
            ("give", 3, mid), ("join", 0, mid), ("take", 2, end), ("give", 2, end), ("join", 1, None),
            ("expert", 2, None), ("take", 3, end), ("give", 3, end), ("join", 2, None), ("expert", 3, None),
            ("join", 3, None),
        ]
    steps = [("expert", 0, None), ("join", 0, None)]
    for k in range(1, depth):
        steps += [("take", k, None), ("give", k, None), ("expert", k, None), ("join", k, None)]
    return steps


def layer_kernel(
    step_ref, route_ref, share_ref, bias_ref, log_ref, skip_ref, x_ref, b_ref, c_ref, gate_ref, resid_ref, wx_ref, wb_ref, wc_ref, ngain_ref, fgain_ref, w_ref,
    sg_ref, su_ref, sd_ref, eg_ref, eu_ref, ed_ref, out_ref,
    step_in, route_in, share_in, bias_in, log_in, skip_in, xin, bin_, cin, gin, rin, wx, wb, wc, ngain, fgain, w_buf, sg_buf, su_buf, sd_buf, eg_buf, eu_buf, ed_buf,
    xh, bh, ch, y_buf, cm_buf, cum_buf, own_last, last_buf, st_buf, f_buf, b_buf, o_buf, c_buf, bef_buf, normed,
    t_buf, info, info_buf, g_buf, x_buf, r_buf, p_buf, q_buf, acc,
    local_sem, h_send, h_recv, l_send, l_recv, f_send, f_recv, b_send, b_recv, o_send, o_recv,
    w_send, w_pass, w_near, w_recv, m_recv, info_send, info_recv, t_send, t_recv, g_send, x_recv, d_send, r_recv, c_send, q_recv,
    *, depth, side, ndp, ways, picks, experts, heads,
):
    tokens, model = t_buf.shape[1:]
    plane, slots = g_buf.shape[1:3]
    groups, wide, state = st_buf.shape
    inner = groups * wide
    per = heads // groups
    width = inner // heads
    share = groups // side
    lanes = plane * slots
    rows = tokens // CHUNKS
    tile = min(512, model)
    sp, dp = lax.axis_index("sp"), lax.axis_index("dp")
    zi, yi = sp // side, sp % side
    me = yi * ndp + dp
    mate = dp + 1 - 2 * (dp % 2)
    order = orders(depth)
    source = [pick(zi, [order[z][k] for z in range(depth)]) for k in range(depth)]

    def peer(q):
        return (zi * side + q // ndp, q % ndp)

    def along(step):
        return (sp + step * side, dp)

    def landed(ref, sem):
        pltpu.make_async_copy(ref, ref, sem).wait()

    def remote(src, dst, send, recv, device):
        pltpu.make_async_remote_copy(
            src_ref=src, dst_ref=dst, send_sem=send, recv_sem=recv, device_id=device, device_id_type=MESH
        ).start()

    local = [
        (x_ref, xin), (b_ref, bin_), (c_ref, cin), (wx_ref, wx), (wb_ref, wb), (wc_ref, wc),
        (step_ref, step_in), (route_ref, route_in), (share_ref, share_in), (bias_ref, bias_in), (log_ref, log_in),
        (skip_ref, skip_in),
        (gate_ref, gin), (ngain_ref, ngain), (w_ref, w_buf.at[dp]), (resid_ref, rin), (fgain_ref, fgain),
        (sg_ref, sg_buf), (su_ref, su_buf), (sd_ref, sd_buf),
        (eg_ref.at[0], eg_buf), (eu_ref.at[0], eu_buf), (ed_ref.at[0], ed_buf),
    ]
    loads = [pltpu.make_async_copy(a, b, local_sem.at[i]) for i, (a, b) in enumerate(local)]
    for c in loads:
        c.start()

    barrier = pltpu.get_barrier_semaphore()

    @pl.loop(1, plane)
    def _(j):
        pl.semaphore_signal(barrier, inc=1, device_id=peer((me + j) % plane), device_id_type=MESH)

    @pl.loop(1, depth)
    def _(j):
        pl.semaphore_signal(
            barrier, inc=1, device_id=((zi + j) % depth * side + sp % side, dp), device_id_type=MESH
        )

    for step in (1, ways - 1):
        pl.semaphore_signal(barrier, inc=1, device_id=((sp + step) % ways, dp), device_id_type=MESH)
    pl.semaphore_wait(barrier, plane - 1 + depth - 1 + 2)

    w_rows = w_buf.shape[1]
    piece = w_rows // PARTS
    quarter = PARTS // 4
    half = (yi + zi) % 2

    def place(which, i):
        return which * 2 * quarter + (i % 2) * quarter + i // 2

    def span_of(n):
        return pl.ds(pl.multiple_of(n * piece, piece), piece)

    for i in range(2 * quarter):
        n = place(half, i)
        for hop in range(2, ndp, 2):
            remote(
                w_ref.at[span_of(n)], w_buf.at[dp, span_of(n)], w_send.at[hop // 2], w_recv.at[dp, n],
                (sp, (dp + hop) % ndp),
            )
    remote(w_ref, w_buf.at[dp], w_send.at[0], m_recv.at[dp], (sp, mate))
    near = (zi * side + yi + 1 - 2 * (yi % 2), sp + (1 - 2 * (zi % 2)) * side)

    def pass_on(held_by, n):
        part = w_buf.at[held_by, span_of(n)]
        remote(part, part, w_pass.at[held_by], w_recv.at[held_by, n], (sp, mate))

    def relay(i):
        n = place(half, i)
        for hop in range(2, ndp, 2):
            held_by = (dp + ndp - hop) % ndp
            part = w_buf.at[held_by, span_of(n)]
            landed(part, w_recv.at[held_by, n])
            remote(part, part, w_near.at[i % 2, held_by], w_recv.at[held_by, n], (near[i % 2], dp))
            pass_on(held_by, n)

    def receive(i):
        n = place(1 - half, i)
        for hop in range(2, ndp, 2):
            held_by = (dp + ndp - hop) % ndp
            landed(w_buf.at[held_by, span_of(n)], w_recv.at[held_by, n])
            pass_on(held_by, n)

    for i in range(3):
        loads[i].wait()
    edge = pl.ds(tokens - TAIL, TAIL)

    @pl.when(sp < ways - 1)
    def _():
        for i, (a, b) in enumerate(((xin, xh), (bin_, bh), (cin, ch))):
            remote(a.at[edge], b, h_send.at[i], h_recv.at[i], (sp + 1, dp))

    for i in range(6, 12):
        loads[i].wait()
    raw = step_in[...].astype(F32).T + bias_in[...]
    rate = -jnp.exp(log_in[...])
    skip = skip_in[...]
    step = jnp.maximum(raw, 0.0) + jnp.log(1.0 + jnp.exp(-jnp.abs(raw)))
    logs = step * rate
    row = lax.broadcasted_iota(jnp.int32, (tokens, tokens), 0)
    col = lax.broadcasted_iota(jnp.int32, (tokens, tokens), 1)
    lower = row >= col
    tril = lower.astype(F32)
    cum = lax.dot_general(tril, logs, (((1,), (0,)), ((), ())), precision=HIGH, preferred_element_type=F32)
    cum_t = lax.dot_general(logs, tril, (((0,), (1,)), ((), ())), precision=HIGH, preferred_element_type=F32)
    cum_buf[...] = cum
    last = cum[tokens - 1 : tokens]
    padded = jnp.concatenate([last, jnp.zeros((1, PACK - heads), F32)], axis=1)
    padded = jnp.broadcast_to(padded, (8, PACK))
    own_last[...] = padded
    last_buf[yi] = padded
    to_end = jnp.exp(last - cum)

    @pl.loop(1, side)
    def _(o):
        to = (yi + o) % side
        remote(own_last, last_buf.at[yi], l_send, l_recv.at[yi], (zi * side + to, dp))

    before = jnp.where(row < col, 1.0, 0.0).astype(BF16)
    label = lax.broadcasted_iota(jnp.int32, (experts, tokens), 0).astype(F32)
    lines, used = [], jnp.zeros((experts, 1), F32)
    for p in range(picks):
        named = route_in[p : p + 1].astype(F32)
        hot = jnp.where(label == named, 1.0, 0.0)
        ahead = jnp.dot(hot.astype(BF16), before, preferred_element_type=F32) + used
        used = used + jnp.sum(hot, axis=1, keepdims=True)
        lines.append(named * slots + jnp.sum(ahead * hot, axis=0, keepdims=True))
    lines += [share_in[...], jnp.zeros((8 - 2 * picks, tokens), F32)]
    listed = jnp.concatenate(lines, axis=0)
    info[...] = listed
    info_buf[zi] = listed

    @pl.loop(1, depth)
    def _(j):
        remote(info, info_buf.at[zi], info_send, info_recv.at[zi], ((zi + j) % depth * side + yi, dp))

    for c in loads[3:6]:
        c.wait()

    @pl.when(sp == 0)
    def _():
        for h in (xh, bh, ch):
            h[...] = jnp.zeros(h.shape, BF16)

    @pl.when(sp > 0)
    def _():
        for i, h in enumerate((xh, bh, ch)):
            landed(h, h_recv.at[i])

    relay(0)
    turns = [o * share + gl for gl in range(share) for o in range(side)]
    for g in turns:
        if g == turns[groups // 2]:
            relay(1)
        xcol = slice(g * wide, (g + 1) * wide)
        bcol = slice(g * state, (g + 1) * state)
        xs = conv_silu(xh[:, xcol], xin[:, xcol], wx[:, xcol])
        bm = conv_silu(bh[:, bcol], bin_[:, bcol], wb[:, bcol]).astype(BF16)
        cm = conv_silu(ch[:, bcol], cin[:, bcol], wc[:, bcol]).astype(BF16)
        cm_buf[:, bcol] = cm
        weighted = xs * spread(step, g * per, per, width)
        ended = (weighted * spread(to_end, g * per, per, width)).astype(BF16)
        fresh = lax.dot_general(ended, bm, (((0,), (0,)), ((), ())), preferred_element_type=F32).astype(BF16)
        st_buf[g] = fresh
        owner, gl = g // share, g % share

        @pl.when(owner != yi)
        def _():
            remote(
                st_buf.at[g], f_buf.at[yi, gl], f_send.at[gl], f_recv.at[yi, gl], (zi * side + owner, dp)
            )

        @pl.when(owner == yi)
        def _():
            f_buf[yi, gl] = fresh

        scores = lax.dot_general(cm, bm, (((1,), (1,)), ((), ())), preferred_element_type=F32)
        scores = jnp.where(lower, scores, 0.0)
        parts = []
        small = weighted.astype(BF16)
        for j in range(per):
            h = g * per + j
            decay = jnp.exp(jnp.minimum(cum[:, h : h + 1] - cum_t[h : h + 1, :], 0.0))
            parts.append(
                jnp.dot((scores * decay).astype(BF16), small[:, j * width : (j + 1) * width],
                        preferred_element_type=F32)
            )
        y_buf[:, xcol] = jnp.concatenate(parts, axis=1) + spread(skip, g * per, per, width) * xs

    relay(2)
    for i in (3, 4, 5):
        @pl.when(zi >= i // 2 - i // 4)
        def _():
            relay(i)

    @pl.loop(1, side)
    def _(o):
        landed(last_buf.at[(yi + o) % side], l_recv.at[(yi + o) % side])

    head = lax.broadcasted_iota(jnp.int32, (wide, PACK), 0) // width
    lane = lax.broadcasted_iota(jnp.int32, (wide, PACK), 1)
    held = [jnp.exp(last_buf[o, 0:1]) for o in range(side)]
    for gl in range(share):
        g = yi * share + gl
        mine = lane == head + g * per
        factors = [jnp.sum(jnp.where(mine, held[o], 0.0), axis=1, keepdims=True) for o in range(side)]
        for o in range(1, side):
            other = (yi + o) % side
            landed(f_buf.at[other, gl], f_recv.at[other, gl])

        @pl.when(zi == 0)
        def _():
            b_buf[gl] = jnp.zeros((wide, state), BF16)

        @pl.when(zi > 0)
        def _():
            landed(b_buf.at[gl], b_recv.at[gl])

        carry = b_buf[gl].astype(F32)
        for o in range(side):
            o_buf[o, gl] = carry.astype(BF16)
            carry = carry * factors[o] + f_buf[o, gl].astype(F32)
        c_buf[gl] = carry.astype(BF16)

        @pl.when(zi < depth - 1)
        def _():
            remote(c_buf.at[gl], b_buf.at[gl], b_send.at[gl], b_recv.at[gl], along(1))

        for o in range(1, side):
            other = (yi + o) % side
            remote(
                o_buf.at[other, gl], bef_buf.at[g], o_send.at[gl], o_recv.at[g], (zi * side + other, dp)
            )
        bef_buf[g] = o_buf[yi, gl]

    for i in (12, 13):
        loads[i].wait()
    for i in (3, 4, 5):
        @pl.when(zi < i // 2 - i // 4)
        def _():
            relay(i)

    grow = jnp.exp(cum_buf[...])
    for g in turns:
        xcol = slice(g * wide, (g + 1) * wide)
        if g == turns[groups // 4]:
            relay(6)
        if g == turns[3 * groups // 4]:
            relay(7)

        @pl.when(g // share != yi)
        def _():
            landed(bef_buf.at[g], o_recv.at[g])

        outer = lax.dot_general(
            cm_buf[:, g * state : (g + 1) * state], bef_buf[g], (((1,), (1,)), ((), ())), preferred_element_type=F32
        )
        v = y_buf[:, xcol] + outer * spread(grow, g * per, per, width)
        v = v * silu(gin[:, xcol].astype(F32))
        v = v * lax.rsqrt(jnp.mean(v * v, axis=1, keepdims=True) + EPS)
        normed[:, xcol] = (v * ngain[:, xcol]).astype(BF16)

    for i in range(14, 17):
        loads[i].wait()
    receive(0)
    receive(1)
    landed(w_buf.at[mate], m_recv.at[mate])

    def product(i, cols):
        start = pl.multiple_of(i * w_rows, w_rows)
        return jnp.dot(normed[:, pl.ds(start, w_rows)], w_buf[i, :, cols], preferred_element_type=F32)

    for n in range(0, model, tile):
        cols = slice(n, n + tile)
        acc[:, cols] = rin[:, cols].astype(F32) + product(dp, cols) + product(mate, cols)
    for i in range(2, 2 * quarter):
        receive(i)
    away = []
    for hop in range(2, ndp, 2):
        away += [(dp + ndp - hop) % ndp, (mate + ndp - hop) % ndp]
        for n in range(PARTS):
            landed(w_buf.at[away[-1], span_of(n)], w_recv.at[away[-1], n])
    square = jnp.zeros((tokens, 1), F32)
    for n in range(0, model, tile):
        cols = slice(n, n + tile)
        total = acc[:, cols]
        for i in away:
            total = total + product(i, cols)
        total = total.astype(BF16).astype(F32)
        acc[:, cols] = total
        square = square + jnp.sum(total * total, axis=1, keepdims=True)
    scale = lax.rsqrt(square / model + EPS)
    for n in range(0, model, tile):
        cols = slice(n, n + tile)
        t_buf[zi, :, cols] = (acc[:, cols] * scale * fgain[:, cols]).astype(BF16)

    def token_copy(s, j, up):
        part = pl.ds(j * rows, rows)
        return pltpu.make_async_remote_copy(
            src_ref=t_buf.at[s, part], dst_ref=t_buf.at[s, part], send_sem=t_send.at[1 if up else 0, s],
            recv_sem=t_recv.at[s, j], device_id=along(1 if up else -1), device_id_type=MESH,
        )

    def sum_copy(s, j, up):
        part = pl.ds(j * rows, rows)
        into = s if up else jnp.where(s == zi - 1, depth, s)
        return pltpu.make_async_remote_copy(
            src_ref=p_buf.at[s, part], dst_ref=q_buf.at[into, part], send_sem=c_send.at[s],
            recv_sem=q_recv.at[into, j], device_id=along(1 if up else -1), device_id_type=MESH,
        )

    def send_sum(s, j):
        @pl.when(s > zi)
        def _():
            sum_copy(s, j, True).start()

        @pl.when(s < zi)
        def _():
            sum_copy(s, j, False).start()

    def send_up(s, j):
        @pl.when((s <= zi) & (zi < depth - 1))
        def _():
            token_copy(s, j, True).start()

    def send_down(s, j):
        @pl.when((s >= zi) & (zi > 0))
        def _():
            token_copy(s, j, False).start()

    def send_tokens(s, j):
        send_up(s, j)
        send_down(s, j)

    def take(k):
        s = source[k]
        landed(info_buf.at[s], info_recv.at[s])
        for j in range(CHUNKS):
            landed(t_buf.at[s, pl.ds(j * rows, rows)], t_recv.at[s, j])
            send_tokens(s, j)

    lag = 3 * CHUNKS // 8

    def pair(k):
        for s in (source[k], source[k + 1]):
            landed(info_buf.at[s], info_recv.at[s])
        for j in range(CHUNKS):
            for s in (source[k], source[k + 1]):
                landed(t_buf.at[s, pl.ds(j * rows, rows)], t_recv.at[s, j])
            send_tokens(source[k], j)

    def late(k):
        for j in range(CHUNKS):
            send_tokens(source[k], j)

    def target():
        row = lax.broadcasted_iota(jnp.int32, (lanes, tokens), 0) + zi * lanes
        return row.astype(F32)

    def give(k):
        s = source[k]
        listing = info_buf[s]
        slot = target()
        chosen = slot == listing[0:1]
        for p in range(1, picks):
            chosen = chosen | (slot == listing[p : p + 1])
        chosen = jnp.where(chosen, 1.0, 0.0).astype(BF16)
        for n in range(0, model, tile):
            cols = slice(n, n + tile)
            part = jnp.dot(chosen, t_buf[s, :, cols], preferred_element_type=F32).astype(BF16)
            g_buf[s, :, :, cols] = part.reshape(plane, slots, tile)

        @pl.loop(1, plane)
        def _(j):
            q = (me + j) % plane
            pltpu.make_async_remote_copy(
                src_ref=g_buf.at[s, q], dst_ref=x_buf.at[s, me], send_sem=g_send.at[s], recv_sem=x_recv.at[s],
                device_id=peer(q), device_id_type=MESH,
            ).start()

        x_buf[s, me] = g_buf[s, me]

    def expert(k):
        s = source[k]
        landed(x_buf.at[s, pl.ds(0, plane - 1)], x_recv.at[s])
        rows_in = x_buf[s].reshape(lanes, model)
        gate = jnp.dot(rows_in, eg_buf[...], preferred_element_type=F32)
        up = jnp.dot(rows_in, eu_buf[...], preferred_element_type=F32)
        hidden = (silu(gate) * up).astype(BF16)
        for n in range(0, model, tile):
            cols = slice(n, n + tile)
            part = jnp.dot(hidden, ed_buf[:, cols], preferred_element_type=F32).astype(BF16)
            x_buf[s, :, :, cols] = part.reshape(plane, slots, tile)

        @pl.loop(1, plane)
        def _(j):
            q = (me + j) % plane
            pltpu.make_async_remote_copy(
                src_ref=x_buf.at[s, q], dst_ref=r_buf.at[s, me], send_sem=d_send.at[s], recv_sem=r_recv.at[s],
                device_id=peer(q), device_id_type=MESH,
            ).start()

        r_buf[s, me] = x_buf[s, me]

    def join(k):
        s = source[k]
        landed(r_buf.at[s, pl.ds(0, plane - 1)], r_recv.at[s])
        listing = info_buf[s]
        slot = target()
        weight = jnp.zeros((lanes, tokens), F32)
        for p in range(picks):
            weight = weight + jnp.where(slot == listing[p : p + 1], listing[picks + p : picks + p + 1], 0.0)
        high = weight.astype(BF16)
        low = (weight - high.astype(F32)).astype(BF16)
        for n in range(0, model, tile):
            cols = slice(n, n + tile)
            block = r_buf[s, :, :, cols].reshape(lanes, tile)
            part = lax.dot_general(high, block, (((0,), (0,)), ((), ())), preferred_element_type=F32)
            part = part + lax.dot_general(low, block, (((0,), (0,)), ((), ())), preferred_element_type=F32)
            if k == 0:
                acc[:, cols] = acc[:, cols] + part
            else:
                p_buf[s, :, cols] = part.astype(BF16)
        if k:
            @pl.when((zi == 0) | (zi == depth - 1))
            def _():
                for j in range(CHUNKS):
                    send_sum(s, j)

    for j in range(CHUNKS):
        send_tokens(zi, j)
    give(0)

    for c in loads[17:20]:
        c.wait()
    x = t_buf[zi]
    hidden = silu(jnp.dot(x, sg_buf[...], preferred_element_type=F32)) * jnp.dot(
        x, su_buf[...], preferred_element_type=F32
    )
    hidden = hidden.astype(BF16)
    for n in range(0, model, tile):
        cols = slice(n, n + tile)
        acc[:, cols] = acc[:, cols] + jnp.dot(hidden, sd_buf[:, cols], preferred_element_type=F32)

    for c in loads[20:]:
        c.wait()

    actions = {"take": take, "pair": pair, "late": late, "give": give, "expert": expert, "join": join}
    for name, k, planes in layer_of_steps(depth):
        if planes is None:
            actions[name](k)
        else:
            taken = zi == planes[0]
            for z in planes[1:]:
                taken = taken | (zi == z)

            @pl.when(taken)
            def _(name=name, k=k):
                actions[name](k)

    def pass_sum(s, j):
        part = pl.ds(j * rows, rows)
        landed(q_buf.at[s, part], q_recv.at[s, j])
        p_buf[s, part] = (p_buf[s, part].astype(F32) + q_buf[s, part].astype(F32)).astype(BF16)
        send_sum(s, j)

    def far(z, s):
        return depth - 1 - s + depth - 1 - z if s < z else s + z

    @pl.when((zi > 0) & (zi < depth - 1))
    def _():
        if depth == 4:
            first, second, third = [pick(zi, [0] + t + [0]) for t in ([3, 0], [0, 3], [2, 1])]
            for j in range(CHUNKS + lag):
                if j < CHUNKS:
                    pass_sum(first, j)
                if j >= lag:
                    pass_sum(second, j - lag)
            for j in range(CHUNKS):
                pass_sum(third, j)
        else:
            passing = [
                sorted((s for s in range(depth) if s != z), key=lambda s, z=z: (far(z, s), s)) for z in range(depth)
            ]
            for i in range(depth - 1):
                for j in range(CHUNKS):
                    pass_sum(pick(zi, [passing[z][i] for z in range(depth)]), j)

    for j in range(CHUNKS):
        part = pl.ds(j * rows, rows)

        @pl.when(zi > 0)
        def _():
            landed(q_buf.at[zi, part], q_recv.at[zi, j])
            acc[part] = acc[part] + q_buf[zi, part].astype(F32)

        @pl.when(zi < depth - 1)
        def _():
            landed(q_buf.at[depth, part], q_recv.at[depth, j])
            acc[part] = acc[part] + q_buf[depth, part].astype(F32)

        out_ref[part] = acc[part].astype(BF16)

    @pl.loop(1, depth)
    def _(j):
        landed(info, info_send)

    @pl.loop(1, side)
    def _(o):
        landed(own_last, l_send)

    @pl.when(sp < ways - 1)
    def _():
        for i, h in enumerate((xh, bh, ch)):
            landed(h, h_send.at[i])

    for gl in range(share):
        for _ in range(1, side):
            landed(st_buf.at[0], f_send.at[gl])
            landed(st_buf.at[0], o_send.at[gl])

        @pl.when(zi < depth - 1)
        def _():
            landed(c_buf.at[gl], b_send.at[gl])

    landed(w_buf.at[0], w_send.at[0])
    for hop in range(2, ndp, 2):
        held_by = (dp + ndp - hop) % ndp
        landed(w_buf.at[0, pl.ds(0, 2 * quarter * piece)], w_send.at[hop // 2])
        landed(w_buf.at[0], w_pass.at[held_by])
        for i in range(2):
            landed(w_buf.at[0, pl.ds(0, quarter * piece)], w_near.at[i, held_by])

    for k in range(depth):
        s = source[k]
        landed(g_buf.at[s, pl.ds(0, plane - 1)], g_send.at[s])
        landed(x_buf.at[s, pl.ds(0, plane - 1)], d_send.at[s])
        if k:
            landed(p_buf.at[s], c_send.at[s])

        @pl.when((s <= zi) & (zi < depth - 1))
        def _():
            landed(t_buf.at[s], t_send.at[1, s])

        @pl.when((s >= zi) & (zi > 0))
        def _():
            landed(t_buf.at[s], t_send.at[0, s])


def vmem(count):
    return [pl.BlockSpec(memory_space=pltpu.VMEM)] * count


def body(
    residual, head_input, gate_input, b_input, c_input, step_input, conv_weight, conv_b_weight,
    conv_c_weight, step_bias, decay_log, skip, norm_gain, out_weight, ffn_gain, shared_gate,
    shared_up, shared_down, expert_gate, expert_up, expert_down, routes, route_weights,
):
    tokens, inner = head_input.shape[1:]
    heads = step_bias.shape[0]
    state = 128
    span = b_input.shape[2]
    groups = span // state
    model = residual.shape[2]
    ways, ndp = lax.axis_size("sp"), lax.axis_size("dp")
    picks = routes.shape[2]
    side = max(1, ndp // 2)
    depth = ways // side
    plane = side * ndp
    experts = ways * ndp
    slots = max(16, 2 * tokens * picks // experts)
    share = groups // side
    wide = inner // groups
    hbm = [pl.BlockSpec(memory_space=pl.ANY)]
    dma = pltpu.SemaphoreType.DMA
    hidden = expert_gate.shape[2]
    shared = shared_gate.shape[1]

    def halves(*shape):
        return pltpu.VMEM(shape, BF16)

    def floats(*shape):
        return pltpu.VMEM(shape, F32)

    out = pl.pallas_call(
        lambda *refs: layer_kernel(
            *refs, depth=depth, side=side, ndp=ndp, ways=ways, picks=picks, experts=experts, heads=heads
        ),
        out_shape=jax.ShapeDtypeStruct((tokens, model), BF16),
        in_specs=hbm * 23,
        out_specs=vmem(1)[0],
        scratch_shapes=[
            halves(heads, tokens), pltpu.VMEM((picks, tokens), jnp.int32), floats(picks, tokens), floats(1, heads),
            floats(1, heads), floats(1, heads), halves(tokens, inner), halves(tokens, span), halves(tokens, span),
            halves(tokens, inner), halves(tokens, model), halves(*conv_weight.shape), halves(*conv_b_weight.shape),
            halves(*conv_c_weight.shape), floats(1, inner), floats(1, model),
            halves(ndp, inner // ndp, model), halves(model, shared), halves(model, shared), halves(shared, model),
            halves(model, hidden), halves(model, hidden), halves(hidden, model),
            halves(TAIL, inner), halves(TAIL, span), halves(TAIL, span), floats(tokens, inner), halves(tokens, span),
            floats(tokens, heads), floats(8, PACK), floats(side, 8, PACK), halves(groups, wide, state),
            halves(side, share, wide, state), halves(share, wide, state), halves(side, share, wide, state),
            halves(share, wide, state), halves(groups, wide, state), halves(tokens, inner),
            halves(depth, tokens, model), floats(8, tokens), floats(depth, 8, tokens),
            halves(depth, plane, slots, model), halves(depth, plane, slots, model), halves(depth, plane, slots, model),
            halves(depth, tokens, model), halves(depth + 1, tokens, model), floats(tokens, model),
            dma((23,)), dma((3,)), dma((3,)), dma, dma((side,)), dma((share,)), dma((side, share)), dma((share,)),
            dma((share,)), dma((share,)), dma((groups,)), dma((max(1, ndp // 2),)), dma((ndp,)),
            dma((2, ndp)), dma((ndp, PARTS)), dma((ndp,)),
            dma, dma((depth,)), dma((2, depth)), dma((depth, CHUNKS)), dma((depth,)), dma((depth,)),
            dma((depth,)), dma((depth,)), dma((depth,)), dma((depth + 1, CHUNKS)),
        ],
        compiler_params=pltpu.CompilerParams(
            vmem_limit_bytes=63 * 1024 * 1024, collective_id=1, has_side_effects=True
        ),
        cost_estimate=pl.CostEstimate(flops=8_000_000_000, bytes_accessed=24_000_000, transcendentals=500_000),
    )(
        step_input[0].T, routes[0].T, route_weights[0].T, step_bias[None], decay_log[None], skip[None], head_input[0], b_input[0], c_input[0], gate_input[0], residual[0], conv_weight, conv_b_weight,
        conv_c_weight, norm_gain[None], ffn_gain[None], out_weight, shared_gate, shared_up, shared_down,
        expert_gate, expert_up, expert_down,
    )
    return out[None]


def solution(mesh):
    rows = P("dp", "sp", None)
    split = P(("sp", "dp"), None, None)
    return jax.shard_map(
        body,
        mesh=mesh,
        in_specs=(rows,) * 6 + (P(),) * 7 + (P("dp", None),) + (P(),) * 4 + (split,) * 3 + (rows,) * 2,
        out_specs=rows,
        check_vma=False,
    )
```

```python
import jax
import jax.numpy as jnp
from jax import lax
from jax.experimental import pallas as pl
from jax.experimental.pallas import tpu as pltpu
from jax.sharding import PartitionSpec as P

EPS = 1e-06
HIGH = lax.Precision.HIGHEST
HALO = 8
TAIL = 16
PACK = 128
F32 = jnp.float32
BF16 = jnp.bfloat16
MESH = pl.DeviceIdType.MESH
CHUNKS = 8
PARTS = 16


def silu(v):
    return v * (1.0 / (1.0 + jnp.exp(-v)))


def conv_silu(halo, rows, taps):
    count = taps.shape[0]
    length = rows.shape[0]
    padded = jnp.concatenate([halo.astype(F32)[-HALO:], rows.astype(F32)], axis=0)
    total = None
    for tap in range(count):
        start = HALO - (count - 1) + tap
        term = padded[start : start + length] * taps[tap : tap + 1].astype(F32)
        total = term if total is None else total + term
    return silu(total)


def spread(columns, first, count, width):
    rows = columns.shape[0]
    return jnp.concatenate(
        [jnp.broadcast_to(columns[:, first + j : first + j + 1], (rows, width)) for j in range(count)],
        axis=1,
    )


def pick(index, table):
    value = jnp.int32(table[0])
    for c in range(1, len(table)):
        value = jnp.where(index == c, jnp.int32(table[c]), value)
    return value


def orders(depth):
    if depth == 4:
        return [[0, 1, 3, 2], [1, 0, 2, 3], [2, 3, 1, 0], [3, 2, 0, 1]]
    return [[z] + sorted((s for s in range(depth) if s != z), key=lambda s: (abs(s - z), s)) for z in range(depth)]


def layer_of_steps(depth):
    if depth == 4:
        mid, end = (1, 2), (0, 3)
        return [
            ("expert", 0, None), ("take", 1, end), ("pair", 1, mid), ("give", 1, None),
            ("give", 2, mid), ("join", 0, end), ("take", 3, mid), ("late", 2, mid), ("expert", 1, None),
            ("give", 3, mid), ("join", 0, mid), ("take", 2, end), ("give", 2, end), ("join", 1, None),
            ("expert", 2, None), ("take", 3, end), ("give", 3, end), ("join", 2, None), ("expert", 3, None),
            ("join", 3, None),
        ]
    steps = [("expert", 0, None), ("join", 0, None)]
    for k in range(1, depth):
        steps += [("take", k, None), ("give", k, None), ("expert", k, None), ("join", k, None)]
    return steps


def layer_kernel(
    step_ref, route_ref, share_ref, bias_ref, log_ref, skip_ref, x_ref, b_ref, c_ref, gate_ref, resid_ref, wx_ref, wb_ref, wc_ref, ngain_ref, fgain_ref, w_ref,
    sg_ref, su_ref, sd_ref, eg_ref, eu_ref, ed_ref, out_ref,
    step_in, route_in, share_in, bias_in, log_in, skip_in, xin, bin_, cin, gin, rin, wx, wb, wc, ngain, fgain, w_buf, sg_buf, su_buf, sd_buf, eg_buf, eu_buf, ed_buf,
    xh, bh, ch, y_buf, cm_buf, bm_buf, small_buf, cum_buf, own_last, last_buf, st_buf, f_buf, b_buf, o_buf, c_buf, bef_buf, normed,
    t_buf, info, info_buf, g_buf, x_buf, r_buf, p_buf, q_buf, acc,
    local_sem, h_send, h_recv, l_send, l_recv, f_send, f_recv, b_send, b_recv, o_send, o_recv,
    w_send, w_pass, w_near, w_recv, m_recv, info_send, info_recv, t_send, t_recv, g_send, x_recv, d_send, r_recv, c_send, q_recv,
    *, depth, side, ndp, ways, picks, experts, heads,
):
    tokens, model = t_buf.shape[1:]
    plane, slots = g_buf.shape[1:3]
    groups, wide, state = st_buf.shape
    inner = groups * wide
    per = heads // groups
    width = inner // heads
    share = groups // side
    lanes = plane * slots
    rows = tokens // CHUNKS
    tile = min(512, model)
    sp, dp = lax.axis_index("sp"), lax.axis_index("dp")
    zi, yi = sp // side, sp % side
    me = yi * ndp + dp
    mate = dp + 1 - 2 * (dp % 2)
    order = orders(depth)
    source = [pick(zi, [order[z][k] for z in range(depth)]) for k in range(depth)]

    def peer(q):
        return (zi * side + q // ndp, q % ndp)

    def along(step):
        return (sp + step * side, dp)

    def landed(ref, sem):
        pltpu.make_async_copy(ref, ref, sem).wait()

    def remote(src, dst, send, recv, device):
        pltpu.make_async_remote_copy(
            src_ref=src, dst_ref=dst, send_sem=send, recv_sem=recv, device_id=device, device_id_type=MESH
        ).start()

    local = [
        (x_ref, xin), (b_ref, bin_), (c_ref, cin), (wx_ref, wx), (wb_ref, wb), (wc_ref, wc),
        (step_ref, step_in), (route_ref, route_in), (share_ref, share_in), (bias_ref, bias_in), (log_ref, log_in),
        (skip_ref, skip_in),
        (gate_ref, gin), (ngain_ref, ngain), (w_ref, w_buf.at[dp]), (resid_ref, rin), (fgain_ref, fgain),
        (sg_ref, sg_buf), (su_ref, su_buf), (sd_ref, sd_buf),
        (eg_ref.at[0], eg_buf), (eu_ref.at[0], eu_buf), (ed_ref.at[0], ed_buf),
    ]
    loads = [pltpu.make_async_copy(a, b, local_sem.at[i]) for i, (a, b) in enumerate(local)]
    for c in loads:
        c.start()

    barrier = pltpu.get_barrier_semaphore()

    @pl.loop(1, plane)
    def _(j):
        pl.semaphore_signal(barrier, inc=1, device_id=peer((me + j) % plane), device_id_type=MESH)

    @pl.loop(1, depth)
    def _(j):
        pl.semaphore_signal(
            barrier, inc=1, device_id=((zi + j) % depth * side + sp % side, dp), device_id_type=MESH
        )

    for step in (1, ways - 1):
        pl.semaphore_signal(barrier, inc=1, device_id=((sp + step) % ways, dp), device_id_type=MESH)
    pl.semaphore_wait(barrier, plane - 1 + depth - 1 + 2)

    w_rows = w_buf.shape[1]
    piece = w_rows // PARTS
    quarter = PARTS // 4
    half = (yi + zi) % 2

    def place(which, i):
        return which * 2 * quarter + (i % 2) * quarter + i // 2

    def span_of(n):
        return pl.ds(pl.multiple_of(n * piece, piece), piece)

    for i in range(2 * quarter):
        n = place(half, i)
        for hop in range(2, ndp, 2):
            remote(
                w_ref.at[span_of(n)], w_buf.at[dp, span_of(n)], w_send.at[hop // 2], w_recv.at[dp, n],
                (sp, (dp + hop) % ndp),
            )
    remote(w_ref, w_buf.at[dp], w_send.at[0], m_recv.at[dp], (sp, mate))
    near = (zi * side + yi + 1 - 2 * (yi % 2), sp + (1 - 2 * (zi % 2)) * side)

    def pass_on(held_by, n):
        part = w_buf.at[held_by, span_of(n)]
        remote(part, part, w_pass.at[held_by], w_recv.at[held_by, n], (sp, mate))

    def relay(i):
        n = place(half, i)
        for hop in range(2, ndp, 2):
            held_by = (dp + ndp - hop) % ndp
            part = w_buf.at[held_by, span_of(n)]
            landed(part, w_recv.at[held_by, n])
            remote(part, part, w_near.at[i % 2, held_by], w_recv.at[held_by, n], (near[i % 2], dp))
            pass_on(held_by, n)

    def receive(i):
        n = place(1 - half, i)
        for hop in range(2, ndp, 2):
            held_by = (dp + ndp - hop) % ndp
            landed(w_buf.at[held_by, span_of(n)], w_recv.at[held_by, n])
            pass_on(held_by, n)

    for i in range(3):
        loads[i].wait()
    edge = pl.ds(tokens - TAIL, TAIL)

    @pl.when(sp < ways - 1)
    def _():
        for i, (a, b) in enumerate(((xin, xh), (bin_, bh), (cin, ch))):
            remote(a.at[edge], b, h_send.at[i], h_recv.at[i], (sp + 1, dp))

    for i in range(6, 12):
        loads[i].wait()
    raw = step_in[...].astype(F32).T + bias_in[...]
    rate = -jnp.exp(log_in[...])
    skip = skip_in[...]
    step = jnp.maximum(raw, 0.0) + jnp.log(1.0 + jnp.exp(-jnp.abs(raw)))
    logs = step * rate
    row = lax.broadcasted_iota(jnp.int32, (tokens, tokens), 0)
    col = lax.broadcasted_iota(jnp.int32, (tokens, tokens), 1)
    lower = row >= col
    tril = lower.astype(F32)
    cum = lax.dot_general(tril, logs, (((1,), (0,)), ((), ())), precision=HIGH, preferred_element_type=F32)
    cum_t = lax.dot_general(logs, tril, (((0,), (1,)), ((), ())), precision=HIGH, preferred_element_type=F32)
    cum_buf[...] = cum
    last = cum[tokens - 1 : tokens]
    padded = jnp.concatenate([last, jnp.zeros((1, PACK - heads), F32)], axis=1)
    padded = jnp.broadcast_to(padded, (8, PACK))
    own_last[...] = padded
    last_buf[yi] = padded
    to_end = jnp.exp(last - cum)

    @pl.loop(1, side)
    def _(o):
        to = (yi + o) % side
        remote(own_last, last_buf.at[yi], l_send, l_recv.at[yi], (zi * side + to, dp))

    before = jnp.where(row < col, 1.0, 0.0).astype(BF16)
    label = lax.broadcasted_iota(jnp.int32, (experts, tokens), 0).astype(F32)
    lines, used = [], jnp.zeros((experts, 1), F32)
    for p in range(picks):
        named = route_in[p : p + 1].astype(F32)
        hot = jnp.where(label == named, 1.0, 0.0)
        ahead = jnp.dot(hot.astype(BF16), before, preferred_element_type=F32) + used
        used = used + jnp.sum(hot, axis=1, keepdims=True)
        lines.append(named * slots + jnp.sum(ahead * hot, axis=0, keepdims=True))
    lines += [share_in[...], jnp.zeros((8 - 2 * picks, tokens), F32)]
    listed = jnp.concatenate(lines, axis=0)
    info[...] = listed
    info_buf[zi] = listed

    @pl.loop(1, depth)
    def _(j):
        remote(info, info_buf.at[zi], info_send, info_recv.at[zi], ((zi + j) % depth * side + yi, dp))

    for c in loads[3:6]:
        c.wait()

    @pl.when(sp == 0)
    def _():
        for h in (xh, bh, ch):
            h[...] = jnp.zeros(h.shape, BF16)

    @pl.when(sp > 0)
    def _():
        for i, h in enumerate((xh, bh, ch)):
            landed(h, h_recv.at[i])

    relay(0)
    turns = [o * share + gl for gl in range(share) for o in range(side)]
    for g in turns:
        if g == turns[groups // 2]:
            relay(1)
        xcol = slice(g * wide, (g + 1) * wide)
        bcol = slice(g * state, (g + 1) * state)
        xs = conv_silu(xh[:, xcol], xin[:, xcol], wx[:, xcol])
        bm = conv_silu(bh[:, bcol], bin_[:, bcol], wb[:, bcol]).astype(BF16)
        cm = conv_silu(ch[:, bcol], cin[:, bcol], wc[:, bcol]).astype(BF16)
        cm_buf[:, bcol] = cm
        weighted = xs * spread(step, g * per, per, width)
        y_buf[:, xcol] = xs
        bm_buf[:, bcol] = bm
        small_buf[:, xcol] = weighted.astype(BF16)
        ended = (weighted * spread(to_end, g * per, per, width)).astype(BF16)
        fresh = lax.dot_general(ended, bm, (((0,), (0,)), ((), ())), preferred_element_type=F32).astype(BF16)
        st_buf[g] = fresh
        owner, gl = g // share, g % share

        @pl.when(owner != yi)
        def _():
            remote(
                st_buf.at[g], f_buf.at[yi, gl], f_send.at[gl], f_recv.at[yi, gl], (zi * side + owner, dp)
            )

        @pl.when(owner == yi)
        def _():
            f_buf[yi, gl] = fresh

    def inside():
        for g in turns:
            xcol = slice(g * wide, (g + 1) * wide)
            bcol = slice(g * state, (g + 1) * state)
            scores = lax.dot_general(
                cm_buf[:, bcol], bm_buf[:, bcol], (((1,), (1,)), ((), ())), preferred_element_type=F32
            )
            scores = jnp.where(lower, scores, 0.0)
            parts = []
            for j in range(per):
                h = g * per + j
                decay = jnp.exp(jnp.minimum(cum[:, h : h + 1] - cum_t[h : h + 1, :], 0.0))
                parts.append(
                    jnp.dot((scores * decay).astype(BF16), small_buf[:, h * width : (h + 1) * width],
                            preferred_element_type=F32)
                )
            y_buf[:, xcol] = jnp.concatenate(parts, axis=1) + spread(skip, g * per, per, width) * y_buf[:, xcol]

    @pl.when(zi > 0)
    def _():
        inside()

    relay(2)
    for i in (3, 4, 5):
        @pl.when(zi >= i - 2)
        def _():
            relay(i)

    @pl.loop(1, side)
    def _(o):
        landed(last_buf.at[(yi + o) % side], l_recv.at[(yi + o) % side])

    head = lax.broadcasted_iota(jnp.int32, (wide, PACK), 0) // width
    lane = lax.broadcasted_iota(jnp.int32, (wide, PACK), 1)
    held = [jnp.exp(last_buf[o, 0:1]) for o in range(side)]
    for gl in range(share):
        g = yi * share + gl
        mine = lane == head + g * per
        factors = [jnp.sum(jnp.where(mine, held[o], 0.0), axis=1, keepdims=True) for o in range(side)]
        for o in range(1, side):
            other = (yi + o) % side
            landed(f_buf.at[other, gl], f_recv.at[other, gl])

        @pl.when(zi == 0)
        def _():
            b_buf[gl] = jnp.zeros((wide, state), BF16)

        @pl.when(zi > 0)
        def _():
            landed(b_buf.at[gl], b_recv.at[gl])

        carry = b_buf[gl].astype(F32)
        for o in range(side):
            o_buf[o, gl] = carry.astype(BF16)
            carry = carry * factors[o] + f_buf[o, gl].astype(F32)
        c_buf[gl] = carry.astype(BF16)

        @pl.when(zi < depth - 1)
        def _():
            remote(c_buf.at[gl], b_buf.at[gl], b_send.at[gl], b_recv.at[gl], along(1))

        for o in range(1, side):
            other = (yi + o) % side
            remote(
                o_buf.at[other, gl], bef_buf.at[g], o_send.at[gl], o_recv.at[g], (zi * side + other, dp)
            )
        bef_buf[g] = o_buf[yi, gl]
        if gl in (0, 1):
            for z in range(1, 4):
                @pl.when(jnp.minimum(zi, 3) == z)
                def _():
                    relay(z + 3 + gl)

    @pl.when(zi == 0)
    def _():
        inside()

    for i in (12, 13):
        loads[i].wait()
    for i in (3, 4, 5):
        @pl.when(zi == 0)
        def _():
            relay(i)

    grow = jnp.exp(cum_buf[...])
    for g in turns:
        xcol = slice(g * wide, (g + 1) * wide)
        if g in (turns[groups // 4], turns[groups // 2]):
            i = 6 if g == turns[groups // 4] else 7

            @pl.when(zi < i - 4)
            def _():
                relay(i)

        @pl.when(g // share != yi)
        def _():
            landed(bef_buf.at[g], o_recv.at[g])

        outer = lax.dot_general(
            cm_buf[:, g * state : (g + 1) * state], bef_buf[g], (((1,), (1,)), ((), ())), preferred_element_type=F32
        )
        v = y_buf[:, xcol] + outer * spread(grow, g * per, per, width)
        v = v * silu(gin[:, xcol].astype(F32))
        v = v * lax.rsqrt(jnp.mean(v * v, axis=1, keepdims=True) + EPS)
        normed[:, xcol] = (v * ngain[:, xcol]).astype(BF16)

    for i in range(14, 17):
        loads[i].wait()
    receive(0)
    receive(1)
    landed(w_buf.at[mate], m_recv.at[mate])

    def product(i, cols):
        start = pl.multiple_of(i * w_rows, w_rows)
        return jnp.dot(normed[:, pl.ds(start, w_rows)], w_buf[i, :, cols], preferred_element_type=F32)

    for n in range(0, model, tile):
        cols = slice(n, n + tile)
        acc[:, cols] = rin[:, cols].astype(F32) + product(dp, cols) + product(mate, cols)
    for i in range(2, 2 * quarter):
        receive(i)
    away = []
    for hop in range(2, ndp, 2):
        away += [(dp + ndp - hop) % ndp, (mate + ndp - hop) % ndp]
        for n in range(PARTS):
            landed(w_buf.at[away[-1], span_of(n)], w_recv.at[away[-1], n])
    square = jnp.zeros((tokens, 1), F32)
    for n in range(0, model, tile):
        cols = slice(n, n + tile)
        total = acc[:, cols]
        for i in away:
            total = total + product(i, cols)
        total = total.astype(BF16).astype(F32)
        acc[:, cols] = total
        square = square + jnp.sum(total * total, axis=1, keepdims=True)
    scale = lax.rsqrt(square / model + EPS)
    for n in range(0, model, tile):
        cols = slice(n, n + tile)
        t_buf[zi, :, cols] = (acc[:, cols] * scale * fgain[:, cols]).astype(BF16)

    def token_copy(s, j, up):
        part = pl.ds(j * rows, rows)
        return pltpu.make_async_remote_copy(
            src_ref=t_buf.at[s, part], dst_ref=t_buf.at[s, part], send_sem=t_send.at[1 if up else 0, s],
            recv_sem=t_recv.at[s, j], device_id=along(1 if up else -1), device_id_type=MESH,
        )

    def sum_copy(s, j, up):
        part = pl.ds(j * rows, rows)
        into = s if up else jnp.where(s == zi - 1, depth, s)
        return pltpu.make_async_remote_copy(
            src_ref=p_buf.at[s, part], dst_ref=q_buf.at[into, part], send_sem=c_send.at[s],
            recv_sem=q_recv.at[into, j], device_id=along(1 if up else -1), device_id_type=MESH,
        )

    def send_sum(s, j):
        @pl.when(s > zi)
        def _():
            sum_copy(s, j, True).start()

        @pl.when(s < zi)
        def _():
            sum_copy(s, j, False).start()

    def send_up(s, j):
        @pl.when((s <= zi) & (zi < depth - 1))
        def _():
            token_copy(s, j, True).start()

    def send_down(s, j):
        @pl.when((s >= zi) & (zi > 0))
        def _():
            token_copy(s, j, False).start()

    def send_tokens(s, j):
        send_up(s, j)
        send_down(s, j)

    def take(k):
        s = source[k]
        landed(info_buf.at[s], info_recv.at[s])
        for j in range(CHUNKS):
            landed(t_buf.at[s, pl.ds(j * rows, rows)], t_recv.at[s, j])
            send_tokens(s, j)

    lag = 3 * CHUNKS // 8

    def pair(k):
        for s in (source[k], source[k + 1]):
            landed(info_buf.at[s], info_recv.at[s])
        for j in range(CHUNKS):
            for s in (source[k], source[k + 1]):
                landed(t_buf.at[s, pl.ds(j * rows, rows)], t_recv.at[s, j])
            send_tokens(source[k], j)

    def late(k):
        for j in range(CHUNKS):
            send_tokens(source[k], j)

    def target():
        row = lax.broadcasted_iota(jnp.int32, (lanes, tokens), 0) + zi * lanes
        return row.astype(F32)

    def give(k):
        s = source[k]
        listing = info_buf[s]
        slot = target()
        chosen = slot == listing[0:1]
        for p in range(1, picks):
            chosen = chosen | (slot == listing[p : p + 1])
        chosen = jnp.where(chosen, 1.0, 0.0).astype(BF16)
        for n in range(0, model, tile):
            cols = slice(n, n + tile)
            part = jnp.dot(chosen, t_buf[s, :, cols], preferred_element_type=F32).astype(BF16)
            g_buf[s, :, :, cols] = part.reshape(plane, slots, tile)

        @pl.loop(1, plane)
        def _(j):
            q = (me + j) % plane
            pltpu.make_async_remote_copy(
                src_ref=g_buf.at[s, q], dst_ref=x_buf.at[s, me], send_sem=g_send.at[s], recv_sem=x_recv.at[s],
                device_id=peer(q), device_id_type=MESH,
            ).start()

        x_buf[s, me] = g_buf[s, me]

    def expert(k):
        s = source[k]
        landed(x_buf.at[s, pl.ds(0, plane - 1)], x_recv.at[s])
        rows_in = x_buf[s].reshape(lanes, model)
        gate = jnp.dot(rows_in, eg_buf[...], preferred_element_type=F32)
        up = jnp.dot(rows_in, eu_buf[...], preferred_element_type=F32)
        hidden = (silu(gate) * up).astype(BF16)
        for n in range(0, model, tile):
            cols = slice(n, n + tile)
            part = jnp.dot(hidden, ed_buf[:, cols], preferred_element_type=F32).astype(BF16)
            x_buf[s, :, :, cols] = part.reshape(plane, slots, tile)

        @pl.loop(1, plane)
        def _(j):
            q = (me + j) % plane
            pltpu.make_async_remote_copy(
                src_ref=x_buf.at[s, q], dst_ref=r_buf.at[s, me], send_sem=d_send.at[s], recv_sem=r_recv.at[s],
                device_id=peer(q), device_id_type=MESH,
            ).start()

        r_buf[s, me] = x_buf[s, me]

    def join(k):
        s = source[k]
        landed(r_buf.at[s, pl.ds(0, plane - 1)], r_recv.at[s])
        listing = info_buf[s]
        slot = target()
        weight = jnp.zeros((lanes, tokens), F32)
        for p in range(picks):
            weight = weight + jnp.where(slot == listing[p : p + 1], listing[picks + p : picks + p + 1], 0.0)
        high = weight.astype(BF16)
        low = (weight - high.astype(F32)).astype(BF16)
        for n in range(0, model, tile):
            cols = slice(n, n + tile)
            block = r_buf[s, :, :, cols].reshape(lanes, tile)
            part = lax.dot_general(high, block, (((0,), (0,)), ((), ())), preferred_element_type=F32)
            part = part + lax.dot_general(low, block, (((0,), (0,)), ((), ())), preferred_element_type=F32)
            if k == 0:
                acc[:, cols] = acc[:, cols] + part
            else:
                p_buf[s, :, cols] = part.astype(BF16)
        if k:
            @pl.when((zi == 0) | (zi == depth - 1))
            def _():
                for j in range(CHUNKS):
                    send_sum(s, j)

    for j in range(CHUNKS):
        send_tokens(zi, j)
    give(0)

    for c in loads[17:20]:
        c.wait()
    x = t_buf[zi]
    hidden = silu(jnp.dot(x, sg_buf[...], preferred_element_type=F32)) * jnp.dot(
        x, su_buf[...], preferred_element_type=F32
    )
    hidden = hidden.astype(BF16)
    for n in range(0, model, tile):
        cols = slice(n, n + tile)
        acc[:, cols] = acc[:, cols] + jnp.dot(hidden, sd_buf[:, cols], preferred_element_type=F32)

    for c in loads[20:]:
        c.wait()

    actions = {"take": take, "pair": pair, "late": late, "give": give, "expert": expert, "join": join}
    for name, k, planes in layer_of_steps(depth):
        if planes is None:
            actions[name](k)
        else:
            taken = zi == planes[0]
            for z in planes[1:]:
                taken = taken | (zi == z)

            @pl.when(taken)
            def _(name=name, k=k):
                actions[name](k)

    def pass_sum(s, j):
        part = pl.ds(j * rows, rows)
        landed(q_buf.at[s, part], q_recv.at[s, j])
        p_buf[s, part] = (p_buf[s, part].astype(F32) + q_buf[s, part].astype(F32)).astype(BF16)
        send_sum(s, j)

    def far(z, s):
        return depth - 1 - s + depth - 1 - z if s < z else s + z

    @pl.when((zi > 0) & (zi < depth - 1))
    def _():
        if depth == 4:
            first, second, third = [pick(zi, [0] + t + [0]) for t in ([3, 0], [0, 3], [2, 1])]
            for j in range(CHUNKS + lag):
                if j < CHUNKS:
                    pass_sum(first, j)
                if j >= lag:
                    pass_sum(second, j - lag)
            for j in range(CHUNKS):
                pass_sum(third, j)
        else:
            passing = [
                sorted((s for s in range(depth) if s != z), key=lambda s, z=z: (far(z, s), s)) for z in range(depth)
            ]
            for i in range(depth - 1):
                for j in range(CHUNKS):
                    pass_sum(pick(zi, [passing[z][i] for z in range(depth)]), j)

    for j in range(CHUNKS):
        part = pl.ds(j * rows, rows)

        @pl.when(zi > 0)
        def _():
            landed(q_buf.at[zi, part], q_recv.at[zi, j])
            acc[part] = acc[part] + q_buf[zi, part].astype(F32)

        @pl.when(zi < depth - 1)
        def _():
            landed(q_buf.at[depth, part], q_recv.at[depth, j])
            acc[part] = acc[part] + q_buf[depth, part].astype(F32)

        out_ref[part] = acc[part].astype(BF16)

    @pl.loop(1, depth)
    def _(j):
        landed(info, info_send)

    @pl.loop(1, side)
    def _(o):
        landed(own_last, l_send)

    @pl.when(sp < ways - 1)
    def _():
        for i, h in enumerate((xh, bh, ch)):
            landed(h, h_send.at[i])

    for gl in range(share):
        for _ in range(1, side):
            landed(st_buf.at[0], f_send.at[gl])
            landed(st_buf.at[0], o_send.at[gl])

        @pl.when(zi < depth - 1)
        def _():
            landed(c_buf.at[gl], b_send.at[gl])

    landed(w_buf.at[0], w_send.at[0])
    for hop in range(2, ndp, 2):
        held_by = (dp + ndp - hop) % ndp
        landed(w_buf.at[0, pl.ds(0, 2 * quarter * piece)], w_send.at[hop // 2])
        landed(w_buf.at[0], w_pass.at[held_by])
        for i in range(2):
            landed(w_buf.at[0, pl.ds(0, quarter * piece)], w_near.at[i, held_by])

    for k in range(depth):
        s = source[k]
        landed(g_buf.at[s, pl.ds(0, plane - 1)], g_send.at[s])
        landed(x_buf.at[s, pl.ds(0, plane - 1)], d_send.at[s])
        if k:
            landed(p_buf.at[s], c_send.at[s])

        @pl.when((s <= zi) & (zi < depth - 1))
        def _():
            landed(t_buf.at[s], t_send.at[1, s])

        @pl.when((s >= zi) & (zi > 0))
        def _():
            landed(t_buf.at[s], t_send.at[0, s])


def vmem(count):
    return [pl.BlockSpec(memory_space=pltpu.VMEM)] * count


def body(
    residual, head_input, gate_input, b_input, c_input, step_input, conv_weight, conv_b_weight,
    conv_c_weight, step_bias, decay_log, skip, norm_gain, out_weight, ffn_gain, shared_gate,
    shared_up, shared_down, expert_gate, expert_up, expert_down, routes, route_weights,
):
    tokens, inner = head_input.shape[1:]
    heads = step_bias.shape[0]
    state = 128
    span = b_input.shape[2]
    groups = span // state
    model = residual.shape[2]
    ways, ndp = lax.axis_size("sp"), lax.axis_size("dp")
    picks = routes.shape[2]
    side = max(1, ndp // 2)
    depth = ways // side
    plane = side * ndp
    experts = ways * ndp
    slots = max(16, 2 * tokens * picks // experts)
    share = groups // side
    wide = inner // groups
    hbm = [pl.BlockSpec(memory_space=pl.ANY)]
    dma = pltpu.SemaphoreType.DMA
    hidden = expert_gate.shape[2]
    shared = shared_gate.shape[1]

    def halves(*shape):
        return pltpu.VMEM(shape, BF16)

    def floats(*shape):
        return pltpu.VMEM(shape, F32)

    out = pl.pallas_call(
        lambda *refs: layer_kernel(
            *refs, depth=depth, side=side, ndp=ndp, ways=ways, picks=picks, experts=experts, heads=heads
        ),
        out_shape=jax.ShapeDtypeStruct((tokens, model), BF16),
        in_specs=hbm * 23,
        out_specs=vmem(1)[0],
        scratch_shapes=[
            halves(heads, tokens), pltpu.VMEM((picks, tokens), jnp.int32), floats(picks, tokens), floats(1, heads),
            floats(1, heads), floats(1, heads), halves(tokens, inner), halves(tokens, span), halves(tokens, span),
            halves(tokens, inner), halves(tokens, model), halves(*conv_weight.shape), halves(*conv_b_weight.shape),
            halves(*conv_c_weight.shape), floats(1, inner), floats(1, model),
            halves(ndp, inner // ndp, model), halves(model, shared), halves(model, shared), halves(shared, model),
            halves(model, hidden), halves(model, hidden), halves(hidden, model),
            halves(TAIL, inner), halves(TAIL, span), halves(TAIL, span), floats(tokens, inner), halves(tokens, span),
            halves(tokens, span), halves(tokens, inner),
            floats(tokens, heads), floats(8, PACK), floats(side, 8, PACK), halves(groups, wide, state),
            halves(side, share, wide, state), halves(share, wide, state), halves(side, share, wide, state),
            halves(share, wide, state), halves(groups, wide, state), halves(tokens, inner),
            halves(depth, tokens, model), floats(8, tokens), floats(depth, 8, tokens),
            halves(depth, plane, slots, model), halves(depth, plane, slots, model), halves(depth, plane, slots, model),
            halves(depth, tokens, model), halves(depth + 1, tokens, model), floats(tokens, model),
            dma((23,)), dma((3,)), dma((3,)), dma, dma((side,)), dma((share,)), dma((side, share)), dma((share,)),
            dma((share,)), dma((share,)), dma((groups,)), dma((max(1, ndp // 2),)), dma((ndp,)),
            dma((2, ndp)), dma((ndp, PARTS)), dma((ndp,)),
            dma, dma((depth,)), dma((2, depth)), dma((depth, CHUNKS)), dma((depth,)), dma((depth,)),
            dma((depth,)), dma((depth,)), dma((depth,)), dma((depth + 1, CHUNKS)),
        ],
        compiler_params=pltpu.CompilerParams(
            vmem_limit_bytes=63 * 1024 * 1024, collective_id=1, has_side_effects=True
        ),
        cost_estimate=pl.CostEstimate(flops=8_000_000_000, bytes_accessed=24_000_000, transcendentals=500_000),
    )(
        step_input[0].T, routes[0].T, route_weights[0].T, step_bias[None], decay_log[None], skip[None], head_input[0], b_input[0], c_input[0], gate_input[0], residual[0], conv_weight, conv_b_weight,
        conv_c_weight, norm_gain[None], ffn_gain[None], out_weight, shared_gate, shared_up, shared_down,
        expert_gate, expert_up, expert_down,
    )
    return out[None]


def solution(mesh):
    rows = P("dp", "sp", None)
    split = P(("sp", "dp"), None, None)
    return jax.shard_map(
        body,
        mesh=mesh,
        in_specs=(rows,) * 6 + (P(),) * 7 + (P("dp", None),) + (P(),) * 4 + (split,) * 3 + (rows,) * 2,
        out_specs=rows,
        check_vma=False,
    )
```

```python
import jax
import jax.numpy as jnp
from jax import lax
from jax.experimental import pallas as pl
from jax.experimental.pallas import tpu as pltpu
from jax.sharding import PartitionSpec as P

EPS = 1e-06
HIGH = lax.Precision.HIGHEST
HALO = 8
TAIL = 16
PACK = 128
F32 = jnp.float32
BF16 = jnp.bfloat16
MESH = pl.DeviceIdType.MESH
CHUNKS = 8
PARTS = 16


def silu(v):
    return v * (1.0 / (1.0 + jnp.exp(-v)))


def conv_silu(halo, rows, taps):
    count = taps.shape[0]
    length = rows.shape[0]
    padded = jnp.concatenate([halo.astype(F32)[-HALO:], rows.astype(F32)], axis=0)
    total = None
    for tap in range(count):
        start = HALO - (count - 1) + tap
        term = padded[start : start + length] * taps[tap : tap + 1].astype(F32)
        total = term if total is None else total + term
    return silu(total)


def spread(columns, first, count, width):
    rows = columns.shape[0]
    return jnp.concatenate(
        [jnp.broadcast_to(columns[:, first + j : first + j + 1], (rows, width)) for j in range(count)],
        axis=1,
    )


def pick(index, table):
    value = jnp.int32(table[0])
    for c in range(1, len(table)):
        value = jnp.where(index == c, jnp.int32(table[c]), value)
    return value


def orders(depth):
    if depth == 4:
        return [[0, 1, 3, 2], [1, 0, 2, 3], [2, 3, 1, 0], [3, 2, 0, 1]]
    return [[z] + sorted((s for s in range(depth) if s != z), key=lambda s: (abs(s - z), s)) for z in range(depth)]


def layer_of_steps(depth):
    if depth == 4:
        mid, end = (1, 2), (0, 3)
        return [
            ("expert", 0, None), ("take", 1, end), ("pair", 1, mid), ("give", 1, None),
            ("give", 2, mid), ("join", 0, end), ("take", 3, mid), ("late", 2, mid), ("expert", 1, None),
            ("give", 3, mid), ("join", 0, mid), ("take", 2, end), ("give", 2, end), ("join", 1, None),
            ("expert", 2, None), ("take", 3, end), ("give", 3, end), ("join", 2, None), ("expert", 3, None),
            ("join", 3, None),
        ]
    steps = [("expert", 0, None), ("join", 0, None)]
    for k in range(1, depth):
        steps += [("take", k, None), ("give", k, None), ("expert", k, None), ("join", k, None)]
    return steps


def layer_kernel(
    step_ref, route_ref, share_ref, bias_ref, log_ref, skip_ref, x_ref, b_ref, c_ref, gate_ref, resid_ref, wx_ref, wb_ref, wc_ref, ngain_ref, fgain_ref, w_ref,
    sg_ref, su_ref, sd_ref, eg_ref, eu_ref, ed_ref, out_ref,
    step_in, route_in, share_in, bias_in, log_in, skip_in, xin, bin_, cin, gin, rin, wx, wb, wc, ngain, fgain, w_buf, sg_buf, su_buf, sd_buf, eg_buf, eu_buf, ed_buf,
    xh, bh, ch, y_buf, cm_buf, bm_buf, small_buf, cum_buf, own_last, last_buf, st_buf, f_buf, b_buf, o_buf, c_buf, bef_buf, normed,
    t_buf, info, info_buf, g_buf, x_buf, r_buf, p_buf, q_buf, acc,
    local_sem, h_send, h_recv, l_send, l_recv, f_send, f_recv, b_send, b_recv, o_send, o_recv,
    w_send, w_pass, w_near, w_recv, m_recv, info_send, info_recv, t_send, t_recv, g_send, x_recv, d_send, r_recv, c_send, q_recv,
    *, depth, side, ndp, ways, picks, experts, heads,
):
    tokens, model = t_buf.shape[1:]
    plane, slots = g_buf.shape[1:3]
    groups, wide, state = st_buf.shape
    inner = groups * wide
    per = heads // groups
    width = inner // heads
    share = groups // side
    lanes = plane * slots
    rows = tokens // CHUNKS
    tile = min(512, model)
    sp, dp = lax.axis_index("sp"), lax.axis_index("dp")
    zi, yi = sp // side, sp % side
    me = yi * ndp + dp
    mate = dp + 1 - 2 * (dp % 2)
    order = orders(depth)
    source = [pick(zi, [order[z][k] for z in range(depth)]) for k in range(depth)]

    def peer(q):
        return (zi * side + q // ndp, q % ndp)

    def along(step):
        return (sp + step * side, dp)

    def landed(ref, sem):
        pltpu.make_async_copy(ref, ref, sem).wait()

    def remote(src, dst, send, recv, device):
        pltpu.make_async_remote_copy(
            src_ref=src, dst_ref=dst, send_sem=send, recv_sem=recv, device_id=device, device_id_type=MESH
        ).start()

    local = [
        (x_ref, xin), (b_ref, bin_), (c_ref, cin), (wx_ref, wx), (wb_ref, wb), (wc_ref, wc),
        (step_ref, step_in), (route_ref, route_in), (share_ref, share_in), (bias_ref, bias_in), (log_ref, log_in),
        (skip_ref, skip_in),
        (gate_ref, gin), (ngain_ref, ngain), (w_ref, w_buf.at[dp]), (resid_ref, rin), (fgain_ref, fgain),
        (sg_ref, sg_buf), (su_ref, su_buf), (sd_ref, sd_buf),
        (eg_ref.at[0], eg_buf), (eu_ref.at[0], eu_buf), (ed_ref.at[0], ed_buf),
    ]
    loads = [pltpu.make_async_copy(a, b, local_sem.at[i]) for i, (a, b) in enumerate(local)]
    for c in loads:
        c.start()

    barrier = pltpu.get_barrier_semaphore()

    @pl.loop(1, plane)
    def _(j):
        pl.semaphore_signal(barrier, inc=1, device_id=peer((me + j) % plane), device_id_type=MESH)

    @pl.loop(1, depth)
    def _(j):
        pl.semaphore_signal(
            barrier, inc=1, device_id=((zi + j) % depth * side + sp % side, dp), device_id_type=MESH
        )

    for step in (1, ways - 1):
        pl.semaphore_signal(barrier, inc=1, device_id=((sp + step) % ways, dp), device_id_type=MESH)
    pl.semaphore_wait(barrier, plane - 1 + depth - 1 + 2)

    w_rows = w_buf.shape[1]
    piece = w_rows // PARTS
    quarter = PARTS // 4
    half = (yi + zi) % 2

    def place(which, i):
        return which * 2 * quarter + (i % 2) * quarter + i // 2

    def span_of(n):
        return pl.ds(pl.multiple_of(n * piece, piece), piece)

    for i in range(2 * quarter):
        n = place(half, i)
        for hop in range(2, ndp, 2):
            remote(
                w_ref.at[span_of(n)], w_buf.at[dp, span_of(n)], w_send.at[hop // 2], w_recv.at[dp, n],
                (sp, (dp + hop) % ndp),
            )
    remote(w_ref, w_buf.at[dp], w_send.at[0], m_recv.at[dp], (sp, mate))
    near = (zi * side + yi + 1 - 2 * (yi % 2), sp + (1 - 2 * (zi % 2)) * side)

    def pass_on(held_by, n):
        part = w_buf.at[held_by, span_of(n)]
        remote(part, part, w_pass.at[held_by], w_recv.at[held_by, n], (sp, mate))

    def relay(i):
        n = place(half, i)
        for hop in range(2, ndp, 2):
            held_by = (dp + ndp - hop) % ndp
            part = w_buf.at[held_by, span_of(n)]
            landed(part, w_recv.at[held_by, n])
            remote(part, part, w_near.at[i % 2, held_by], w_recv.at[held_by, n], (near[i % 2], dp))
            pass_on(held_by, n)

    def receive(i):
        n = place(1 - half, i)
        for hop in range(2, ndp, 2):
            held_by = (dp + ndp - hop) % ndp
            landed(w_buf.at[held_by, span_of(n)], w_recv.at[held_by, n])
            pass_on(held_by, n)

    for i in range(3):
        loads[i].wait()
    edge = pl.ds(tokens - TAIL, TAIL)

    @pl.when(sp < ways - 1)
    def _():
        for i, (a, b) in enumerate(((xin, xh), (bin_, bh), (cin, ch))):
            remote(a.at[edge], b, h_send.at[i], h_recv.at[i], (sp + 1, dp))

    for i in range(6, 12):
        loads[i].wait()
    raw = step_in[...].astype(F32).T + bias_in[...]
    rate = -jnp.exp(log_in[...])
    skip = skip_in[...]
    step = jnp.maximum(raw, 0.0) + jnp.log(1.0 + jnp.exp(-jnp.abs(raw)))
    logs = step * rate
    row = lax.broadcasted_iota(jnp.int32, (tokens, tokens), 0)
    col = lax.broadcasted_iota(jnp.int32, (tokens, tokens), 1)
    lower = row >= col
    tril = lower.astype(F32)
    cum = lax.dot_general(tril, logs, (((1,), (0,)), ((), ())), precision=HIGH, preferred_element_type=F32)
    cum_t = lax.dot_general(logs, tril, (((0,), (1,)), ((), ())), precision=HIGH, preferred_element_type=F32)
    cum_buf[...] = cum
    last = cum[tokens - 1 : tokens]
    padded = jnp.concatenate([last, jnp.zeros((1, PACK - heads), F32)], axis=1)
    padded = jnp.broadcast_to(padded, (8, PACK))
    own_last[...] = padded
    last_buf[yi] = padded
    to_end = jnp.exp(last - cum)

    @pl.loop(1, side)
    def _(o):
        to = (yi + o) % side
        remote(own_last, last_buf.at[yi], l_send, l_recv.at[yi], (zi * side + to, dp))

    before = jnp.where(row < col, 1.0, 0.0).astype(BF16)
    label = lax.broadcasted_iota(jnp.int32, (experts, tokens), 0).astype(F32)
    lines, used = [], jnp.zeros((experts, 1), F32)
    for p in range(picks):
        named = route_in[p : p + 1].astype(F32)
        hot = jnp.where(label == named, 1.0, 0.0)
        ahead = jnp.dot(hot.astype(BF16), before, preferred_element_type=F32) + used
        used = used + jnp.sum(hot, axis=1, keepdims=True)
        lines.append(named * slots + jnp.sum(ahead * hot, axis=0, keepdims=True))
    lines += [share_in[...], jnp.zeros((8 - 2 * picks, tokens), F32)]
    listed = jnp.concatenate(lines, axis=0)
    info[...] = listed
    info_buf[zi] = listed

    @pl.loop(1, depth)
    def _(j):
        remote(info, info_buf.at[zi], info_send, info_recv.at[zi], ((zi + j) % depth * side + yi, dp))

    for c in loads[3:6]:
        c.wait()

    @pl.when(sp == 0)
    def _():
        for h in (xh, bh, ch):
            h[...] = jnp.zeros(h.shape, BF16)

    @pl.when(sp > 0)
    def _():
        for i, h in enumerate((xh, bh, ch)):
            landed(h, h_recv.at[i])

    relay(0)
    turns = [o * share + gl for gl in range(share) for o in range(side)]
    for g in turns:
        if g == turns[groups // 2]:
            relay(1)
        xcol = slice(g * wide, (g + 1) * wide)
        bcol = slice(g * state, (g + 1) * state)
        xs = conv_silu(xh[:, xcol], xin[:, xcol], wx[:, xcol])
        bm = conv_silu(bh[:, bcol], bin_[:, bcol], wb[:, bcol]).astype(BF16)
        cm = conv_silu(ch[:, bcol], cin[:, bcol], wc[:, bcol]).astype(BF16)
        cm_buf[:, bcol] = cm
        weighted = xs * spread(step, g * per, per, width)
        y_buf[:, xcol] = xs
        bm_buf[:, bcol] = bm
        small_buf[:, xcol] = weighted.astype(BF16)
        ended = (weighted * spread(to_end, g * per, per, width)).astype(BF16)
        fresh = lax.dot_general(ended, bm, (((0,), (0,)), ((), ())), preferred_element_type=F32).astype(BF16)
        st_buf[g] = fresh
        owner, gl = g // share, g % share

        @pl.when(owner != yi)
        def _():
            remote(
                st_buf.at[g], f_buf.at[yi, gl], f_send.at[gl], f_recv.at[yi, gl], (zi * side + owner, dp)
            )

        @pl.when(owner == yi)
        def _():
            f_buf[yi, gl] = fresh

    def inside():
        for g in turns:
            xcol = slice(g * wide, (g + 1) * wide)
            bcol = slice(g * state, (g + 1) * state)
            scores = lax.dot_general(
                cm_buf[:, bcol], bm_buf[:, bcol], (((1,), (1,)), ((), ())), preferred_element_type=F32
            )
            scores = jnp.where(lower, scores, 0.0)
            parts = []
            for j in range(per):
                h = g * per + j
                decay = jnp.exp(jnp.minimum(cum[:, h : h + 1] - cum_t[h : h + 1, :], 0.0))
                parts.append(
                    jnp.dot((scores * decay).astype(BF16), small_buf[:, h * width : (h + 1) * width],
                            preferred_element_type=F32)
                )
            y_buf[:, xcol] = jnp.concatenate(parts, axis=1) + spread(skip, g * per, per, width) * y_buf[:, xcol]

    @pl.when(zi > 0)
    def _():
        inside()

    relay(2)
    for i in (3, 4, 5):
        @pl.when(zi >= i - 2)
        def _():
            relay(i)

    @pl.loop(1, side)
    def _(o):
        landed(last_buf.at[(yi + o) % side], l_recv.at[(yi + o) % side])

    head = lax.broadcasted_iota(jnp.int32, (wide, PACK), 0) // width
    lane = lax.broadcasted_iota(jnp.int32, (wide, PACK), 1)
    held = [jnp.exp(last_buf[o, 0:1]) for o in range(side)]
    for gl in range(share):
        g = yi * share + gl
        mine = lane == head + g * per
        factors = [jnp.sum(jnp.where(mine, held[o], 0.0), axis=1, keepdims=True) for o in range(side)]
        for o in range(1, side):
            other = (yi + o) % side
            landed(f_buf.at[other, gl], f_recv.at[other, gl])

        @pl.when(zi == 0)
        def _():
            b_buf[gl] = jnp.zeros((wide, state), BF16)

        @pl.when(zi > 0)
        def _():
            landed(b_buf.at[gl], b_recv.at[gl])

        carry = b_buf[gl].astype(F32)
        for o in range(side):
            o_buf[o, gl] = carry.astype(BF16)
            carry = carry * factors[o] + f_buf[o, gl].astype(F32)
        c_buf[gl] = carry.astype(BF16)

        @pl.when(zi < depth - 1)
        def _():
            remote(c_buf.at[gl], b_buf.at[gl], b_send.at[gl], b_recv.at[gl], along(1))

        for o in range(1, side):
            other = (yi + o) % side
            remote(
                o_buf.at[other, gl], bef_buf.at[g], o_send.at[gl], o_recv.at[g], (zi * side + other, dp)
            )
        bef_buf[g] = o_buf[yi, gl]
        if gl in (0, 1):
            for z, i in ((1, 4 + gl), (3, 6 + gl)) + ((2, 6),) * gl:
                @pl.when(jnp.minimum(zi, 3) == z)
                def _():
                    relay(i)

    @pl.when(zi == 2)
    def _():
        relay(5)
        relay(7)

    @pl.when(zi == 0)
    def _():
        inside()

    for i in (12, 13):
        loads[i].wait()
    for i in (3, 4, 5):
        @pl.when(zi == 0)
        def _():
            relay(i)

    grow = jnp.exp(cum_buf[...])
    for g in turns:
        xcol = slice(g * wide, (g + 1) * wide)
        if g in (turns[groups // 4], turns[groups // 2]):
            i = 6 if g == turns[groups // 4] else 7

            @pl.when(zi < 2)
            def _():
                relay(i)

        @pl.when(g // share != yi)
        def _():
            landed(bef_buf.at[g], o_recv.at[g])

        outer = lax.dot_general(
            cm_buf[:, g * state : (g + 1) * state], bef_buf[g], (((1,), (1,)), ((), ())), preferred_element_type=F32
        )
        v = y_buf[:, xcol] + outer * spread(grow, g * per, per, width)
        v = v * silu(gin[:, xcol].astype(F32))
        v = v * lax.rsqrt(jnp.mean(v * v, axis=1, keepdims=True) + EPS)
        normed[:, xcol] = (v * ngain[:, xcol]).astype(BF16)

    for i in range(14, 17):
        loads[i].wait()
    receive(0)
    receive(1)
    landed(w_buf.at[mate], m_recv.at[mate])

    def product(i, cols):
        start = pl.multiple_of(i * w_rows, w_rows)
        return jnp.dot(normed[:, pl.ds(start, w_rows)], w_buf[i, :, cols], preferred_element_type=F32)

    for n in range(0, model, tile):
        cols = slice(n, n + tile)
        acc[:, cols] = rin[:, cols].astype(F32) + product(dp, cols) + product(mate, cols)
    for i in range(2, 2 * quarter):
        receive(i)
    away = []
    for hop in range(2, ndp, 2):
        away += [(dp + ndp - hop) % ndp, (mate + ndp - hop) % ndp]
        for n in range(PARTS):
            landed(w_buf.at[away[-1], span_of(n)], w_recv.at[away[-1], n])
    square = jnp.zeros((tokens, 1), F32)
    for n in range(0, model, tile):
        cols = slice(n, n + tile)
        total = acc[:, cols]
        for i in away:
            total = total + product(i, cols)
        total = total.astype(BF16).astype(F32)
        acc[:, cols] = total
        square = square + jnp.sum(total * total, axis=1, keepdims=True)
    scale = lax.rsqrt(square / model + EPS)
    for n in range(0, model, tile):
        cols = slice(n, n + tile)
        t_buf[zi, :, cols] = (acc[:, cols] * scale * fgain[:, cols]).astype(BF16)

    def token_copy(s, j, up):
        part = pl.ds(j * rows, rows)
        return pltpu.make_async_remote_copy(
            src_ref=t_buf.at[s, part], dst_ref=t_buf.at[s, part], send_sem=t_send.at[1 if up else 0, s],
            recv_sem=t_recv.at[s, j], device_id=along(1 if up else -1), device_id_type=MESH,
        )

    def sum_copy(s, j, up):
        part = pl.ds(j * rows, rows)
        into = s if up else jnp.where(s == zi - 1, depth, s)
        return pltpu.make_async_remote_copy(
            src_ref=p_buf.at[s, part], dst_ref=q_buf.at[into, part], send_sem=c_send.at[s],
            recv_sem=q_recv.at[into, j], device_id=along(1 if up else -1), device_id_type=MESH,
        )

    def send_sum(s, j):
        @pl.when(s > zi)
        def _():
            sum_copy(s, j, True).start()

        @pl.when(s < zi)
        def _():
            sum_copy(s, j, False).start()

    def send_up(s, j):
        @pl.when((s <= zi) & (zi < depth - 1))
        def _():
            token_copy(s, j, True).start()

    def send_down(s, j):
        @pl.when((s >= zi) & (zi > 0))
        def _():
            token_copy(s, j, False).start()

    def send_tokens(s, j):
        send_up(s, j)
        send_down(s, j)

    def take(k):
        s = source[k]
        landed(info_buf.at[s], info_recv.at[s])
        for j in range(CHUNKS):
            landed(t_buf.at[s, pl.ds(j * rows, rows)], t_recv.at[s, j])
            send_tokens(s, j)

    lag = 3 * CHUNKS // 8

    def pair(k):
        for s in (source[k], source[k + 1]):
            landed(info_buf.at[s], info_recv.at[s])
        for j in range(CHUNKS):
            for s in (source[k], source[k + 1]):
                landed(t_buf.at[s, pl.ds(j * rows, rows)], t_recv.at[s, j])
            send_tokens(source[k], j)

    def late(k):
        for j in range(CHUNKS):
            send_tokens(source[k], j)

    def target():
        row = lax.broadcasted_iota(jnp.int32, (lanes, tokens), 0) + zi * lanes
        return row.astype(F32)

    def give(k):
        s = source[k]
        listing = info_buf[s]
        slot = target()
        chosen = slot == listing[0:1]
        for p in range(1, picks):
            chosen = chosen | (slot == listing[p : p + 1])
        chosen = jnp.where(chosen, 1.0, 0.0).astype(BF16)
        for n in range(0, model, tile):
            cols = slice(n, n + tile)
            part = jnp.dot(chosen, t_buf[s, :, cols], preferred_element_type=F32).astype(BF16)
            g_buf[s, :, :, cols] = part.reshape(plane, slots, tile)

        @pl.loop(1, plane)
        def _(j):
            q = (me + j) % plane
            pltpu.make_async_remote_copy(
                src_ref=g_buf.at[s, q], dst_ref=x_buf.at[s, me], send_sem=g_send.at[s], recv_sem=x_recv.at[s],
                device_id=peer(q), device_id_type=MESH,
            ).start()

        x_buf[s, me] = g_buf[s, me]

    def expert(k):
        s = source[k]
        landed(x_buf.at[s, pl.ds(0, plane - 1)], x_recv.at[s])
        rows_in = x_buf[s].reshape(lanes, model)
        gate = jnp.dot(rows_in, eg_buf[...], preferred_element_type=F32)
        up = jnp.dot(rows_in, eu_buf[...], preferred_element_type=F32)
        hidden = (silu(gate) * up).astype(BF16)
        for n in range(0, model, tile):
            cols = slice(n, n + tile)
            part = jnp.dot(hidden, ed_buf[:, cols], preferred_element_type=F32).astype(BF16)
            x_buf[s, :, :, cols] = part.reshape(plane, slots, tile)

        @pl.loop(1, plane)
        def _(j):
            q = (me + j) % plane
            pltpu.make_async_remote_copy(
                src_ref=x_buf.at[s, q], dst_ref=r_buf.at[s, me], send_sem=d_send.at[s], recv_sem=r_recv.at[s],
                device_id=peer(q), device_id_type=MESH,
            ).start()

        r_buf[s, me] = x_buf[s, me]

    def join(k):
        s = source[k]
        landed(r_buf.at[s, pl.ds(0, plane - 1)], r_recv.at[s])
        listing = info_buf[s]
        slot = target()
        weight = jnp.zeros((lanes, tokens), F32)
        for p in range(picks):
            weight = weight + jnp.where(slot == listing[p : p + 1], listing[picks + p : picks + p + 1], 0.0)
        high = weight.astype(BF16)
        low = (weight - high.astype(F32)).astype(BF16)
        for n in range(0, model, tile):
            cols = slice(n, n + tile)
            block = r_buf[s, :, :, cols].reshape(lanes, tile)
            part = lax.dot_general(high, block, (((0,), (0,)), ((), ())), preferred_element_type=F32)
            part = part + lax.dot_general(low, block, (((0,), (0,)), ((), ())), preferred_element_type=F32)
            if k == 0:
                acc[:, cols] = acc[:, cols] + part
            else:
                p_buf[s, :, cols] = part.astype(BF16)
        if k:
            @pl.when((zi == 0) | (zi == depth - 1))
            def _():
                for j in range(CHUNKS):
                    send_sum(s, j)

    for j in range(CHUNKS):
        send_tokens(zi, j)
    give(0)

    for c in loads[17:20]:
        c.wait()
    x = t_buf[zi]
    hidden = silu(jnp.dot(x, sg_buf[...], preferred_element_type=F32)) * jnp.dot(
        x, su_buf[...], preferred_element_type=F32
    )
    hidden = hidden.astype(BF16)
    for n in range(0, model, tile):
        cols = slice(n, n + tile)
        acc[:, cols] = acc[:, cols] + jnp.dot(hidden, sd_buf[:, cols], preferred_element_type=F32)

    for c in loads[20:]:
        c.wait()

    actions = {"take": take, "pair": pair, "late": late, "give": give, "expert": expert, "join": join}
    for name, k, planes in layer_of_steps(depth):
        if planes is None:
            actions[name](k)
        else:
            taken = zi == planes[0]
            for z in planes[1:]:
                taken = taken | (zi == z)

            @pl.when(taken)
            def _(name=name, k=k):
                actions[name](k)

    def pass_sum(s, j):
        part = pl.ds(j * rows, rows)
        landed(q_buf.at[s, part], q_recv.at[s, j])
        p_buf[s, part] = (p_buf[s, part].astype(F32) + q_buf[s, part].astype(F32)).astype(BF16)
        send_sum(s, j)

    def far(z, s):
        return depth - 1 - s + depth - 1 - z if s < z else s + z

    @pl.when((zi > 0) & (zi < depth - 1))
    def _():
        if depth == 4:
            first, second, third = [pick(zi, [0] + t + [0]) for t in ([3, 0], [0, 3], [2, 1])]
            for j in range(CHUNKS + lag):
                if j < CHUNKS:
                    pass_sum(first, j)
                if j >= lag:
                    pass_sum(second, j - lag)
            for j in range(CHUNKS):
                pass_sum(third, j)
        else:
            passing = [
                sorted((s for s in range(depth) if s != z), key=lambda s, z=z: (far(z, s), s)) for z in range(depth)
            ]
            for i in range(depth - 1):
                for j in range(CHUNKS):
                    pass_sum(pick(zi, [passing[z][i] for z in range(depth)]), j)

    for j in range(CHUNKS):
        part = pl.ds(j * rows, rows)

        @pl.when(zi > 0)
        def _():
            landed(q_buf.at[zi, part], q_recv.at[zi, j])
            acc[part] = acc[part] + q_buf[zi, part].astype(F32)

        @pl.when(zi < depth - 1)
        def _():
            landed(q_buf.at[depth, part], q_recv.at[depth, j])
            acc[part] = acc[part] + q_buf[depth, part].astype(F32)

        out_ref[part] = acc[part].astype(BF16)

    @pl.loop(1, depth)
    def _(j):
        landed(info, info_send)

    @pl.loop(1, side)
    def _(o):
        landed(own_last, l_send)

    @pl.when(sp < ways - 1)
    def _():
        for i, h in enumerate((xh, bh, ch)):
            landed(h, h_send.at[i])

    for gl in range(share):
        for _ in range(1, side):
            landed(st_buf.at[0], f_send.at[gl])
            landed(st_buf.at[0], o_send.at[gl])

        @pl.when(zi < depth - 1)
        def _():
            landed(c_buf.at[gl], b_send.at[gl])

    landed(w_buf.at[0], w_send.at[0])
    for hop in range(2, ndp, 2):
        held_by = (dp + ndp - hop) % ndp
        landed(w_buf.at[0, pl.ds(0, 2 * quarter * piece)], w_send.at[hop // 2])
        landed(w_buf.at[0], w_pass.at[held_by])
        for i in range(2):
            landed(w_buf.at[0, pl.ds(0, quarter * piece)], w_near.at[i, held_by])

    for k in range(depth):
        s = source[k]
        landed(g_buf.at[s, pl.ds(0, plane - 1)], g_send.at[s])
        landed(x_buf.at[s, pl.ds(0, plane - 1)], d_send.at[s])
        if k:
            landed(p_buf.at[s], c_send.at[s])

        @pl.when((s <= zi) & (zi < depth - 1))
        def _():
            landed(t_buf.at[s], t_send.at[1, s])

        @pl.when((s >= zi) & (zi > 0))
        def _():
            landed(t_buf.at[s], t_send.at[0, s])


def vmem(count):
    return [pl.BlockSpec(memory_space=pltpu.VMEM)] * count


def body(
    residual, head_input, gate_input, b_input, c_input, step_input, conv_weight, conv_b_weight,
    conv_c_weight, step_bias, decay_log, skip, norm_gain, out_weight, ffn_gain, shared_gate,
    shared_up, shared_down, expert_gate, expert_up, expert_down, routes, route_weights,
):
    tokens, inner = head_input.shape[1:]
    heads = step_bias.shape[0]
    state = 128
    span = b_input.shape[2]
    groups = span // state
    model = residual.shape[2]
    ways, ndp = lax.axis_size("sp"), lax.axis_size("dp")
    picks = routes.shape[2]
    side = max(1, ndp // 2)
    depth = ways // side
    plane = side * ndp
    experts = ways * ndp
    slots = max(16, 2 * tokens * picks // experts)
    share = groups // side
    wide = inner // groups
    hbm = [pl.BlockSpec(memory_space=pl.ANY)]
    dma = pltpu.SemaphoreType.DMA
    hidden = expert_gate.shape[2]
    shared = shared_gate.shape[1]

    def halves(*shape):
        return pltpu.VMEM(shape, BF16)

    def floats(*shape):
        return pltpu.VMEM(shape, F32)

    out = pl.pallas_call(
        lambda *refs: layer_kernel(
            *refs, depth=depth, side=side, ndp=ndp, ways=ways, picks=picks, experts=experts, heads=heads
        ),
        out_shape=jax.ShapeDtypeStruct((tokens, model), BF16),
        in_specs=hbm * 23,
        out_specs=vmem(1)[0],
        scratch_shapes=[
            halves(heads, tokens), pltpu.VMEM((picks, tokens), jnp.int32), floats(picks, tokens), floats(1, heads),
            floats(1, heads), floats(1, heads), halves(tokens, inner), halves(tokens, span), halves(tokens, span),
            halves(tokens, inner), halves(tokens, model), halves(*conv_weight.shape), halves(*conv_b_weight.shape),
            halves(*conv_c_weight.shape), floats(1, inner), floats(1, model),
            halves(ndp, inner // ndp, model), halves(model, shared), halves(model, shared), halves(shared, model),
            halves(model, hidden), halves(model, hidden), halves(hidden, model),
            halves(TAIL, inner), halves(TAIL, span), halves(TAIL, span), floats(tokens, inner), halves(tokens, span),
            halves(tokens, span), halves(tokens, inner),
            floats(tokens, heads), floats(8, PACK), floats(side, 8, PACK), halves(groups, wide, state),
            halves(side, share, wide, state), halves(share, wide, state), halves(side, share, wide, state),
            halves(share, wide, state), halves(groups, wide, state), halves(tokens, inner),
            halves(depth, tokens, model), floats(8, tokens), floats(depth, 8, tokens),
            halves(depth, plane, slots, model), halves(depth, plane, slots, model), halves(depth, plane, slots, model),
            halves(depth, tokens, model), halves(depth + 1, tokens, model), floats(tokens, model),
            dma((23,)), dma((3,)), dma((3,)), dma, dma((side,)), dma((share,)), dma((side, share)), dma((share,)),
            dma((share,)), dma((share,)), dma((groups,)), dma((max(1, ndp // 2),)), dma((ndp,)),
            dma((2, ndp)), dma((ndp, PARTS)), dma((ndp,)),
            dma, dma((depth,)), dma((2, depth)), dma((depth, CHUNKS)), dma((depth,)), dma((depth,)),
            dma((depth,)), dma((depth,)), dma((depth,)), dma((depth + 1, CHUNKS)),
        ],
        compiler_params=pltpu.CompilerParams(
            vmem_limit_bytes=63 * 1024 * 1024, collective_id=1, has_side_effects=True
        ),
        cost_estimate=pl.CostEstimate(flops=8_000_000_000, bytes_accessed=24_000_000, transcendentals=500_000),
    )(
        step_input[0].T, routes[0].T, route_weights[0].T, step_bias[None], decay_log[None], skip[None], head_input[0], b_input[0], c_input[0], gate_input[0], residual[0], conv_weight, conv_b_weight,
        conv_c_weight, norm_gain[None], ffn_gain[None], out_weight, shared_gate, shared_up, shared_down,
        expert_gate, expert_up, expert_down,
    )
    return out[None]


def solution(mesh):
    rows = P("dp", "sp", None)
    split = P(("sp", "dp"), None, None)
    return jax.shard_map(
        body,
        mesh=mesh,
        in_specs=(rows,) * 6 + (P(),) * 7 + (P("dp", None),) + (P(),) * 4 + (split,) * 3 + (rows,) * 2,
        out_specs=rows,
        check_vma=False,
    )
```
